512 devices in a mesh: sp: 16 (over z), dp: 32 (over y, x, core).
Axes of the slice: x: 4, y: 4, z: 16, core: 2. Of those that a mesh axis runs over, the one named last changes fastest.
Arguments:
- tokens: bfloat16 [32, 3072, 2048], P('dp', 'sp'), may hold values from -36 to 36
- query_weight: bfloat16 [2048, 2048], P('dp'), may hold values from -0.125 to 0.125
- key_weight: bfloat16 [2048, 512], P('dp'), may hold values from -0.125 to 0.125
- value_weight: bfloat16 [2048, 512], P('dp'), may hold values from -0.125 to 0.125
- forget_weight: bfloat16 [2048, 16], replicated, may hold values from -0.125 to 0.125
- forget_bias: float32 [16], replicated, may hold values from 3.4 to 9
Outputs:
- mixed: bfloat16 [32, 3072, 2048], P('dp', 'sp')
The draws below stay inside these ranges and needn't reach their ends.
All inputs are finite; a program needn't handle non-finite values.
Results may differ from the reference program's by a relative error of at most 0.012.
Values may be sent and summed in bfloat16 or wider, within the bound.
A program may use at most 64 MiB of HBM per device.

```python
import math
import jax
import jax.numpy as jnp
from jax import lax

D = 2048
H = 16
DH = 128
KV = 4
SEQ = 3072
NSEQ = 32


def draw_tokens(key, part):
    base_values = jnp.clip(jax.random.normal(key, (NSEQ, SEQ, D), jnp.float32), -4.0, 4.0)
    return base_values.astype(jnp.bfloat16)


def draw_forget_bias(key, part):
    fast_share = 0.5
    fast_heads = jax.random.uniform(jax.random.fold_in(key, 3), (H,)) < fast_share
    jitter = jax.random.uniform(jax.random.fold_in(key, 5), (H,), jnp.float32)
    return jnp.where(fast_heads, 3.4 + 0.8 * jitter, math.log(SEQ) + 0.4 * jitter).astype(jnp.float32)


def shard_levels(rng, extent, pieces, low, high):
    loudness, own = 1.0, jax.random.fold_in(rng, 6)
    for position, blocks in pieces:
        steps = jnp.exp(jax.random.uniform(jax.random.fold_in(own, position), (blocks,), jnp.float32, low / len(pieces), high / len(pieces)))
        loudness = loudness * jnp.repeat(steps, extent[position] // blocks).reshape([-1 if axis == position else 1 for axis in range(len(extent))])
    return loudness


def centred(key, extent, deviation, reach, shards=(), kind=jnp.bfloat16):
    drawn = deviation * jax.random.normal(key, extent, jnp.float32)
    if shards:
        drawn = drawn * shard_levels(key, extent, shards, -0.22, 0.18)
    return jnp.clip(drawn, -reach, reach).astype(kind)


def setup_inputs(seed: int = 0) -> dict:
    key_list = jax.random.split(jax.random.key(seed), 7)
    return {
        "tokens": draw_tokens(jax.random.fold_in(key_list[6], 71), 0),
        "query_weight": centred(key_list[1], (D, H * DH), D ** -0.5, 0.125, ((0, 32),)),
        "key_weight": centred(key_list[2], (D, KV * DH), D ** -0.5, 0.125, ((0, 32),)),
        "value_weight": centred(key_list[3], (D, KV * DH), D ** -0.5, 0.125, ((0, 32),)),
        "forget_weight": centred(key_list[4], (D, H), D ** -0.5, 0.125),
        "forget_bias": draw_forget_bias(jax.random.fold_in(key_list[6], 71), 0),
    }


def pick_block(length):
    for candidate in (512, 384, 256, 128):
        if length % candidate == 0:
            return candidate
    return length


def reference(tokens, query_weight, key_weight, value_weight, forget_weight, forget_bias):
    seq_count, seq_length, model_width = tokens.shape
    head_count = forget_weight.shape[1]
    head_dim = query_weight.shape[1] // head_count
    key_heads = key_weight.shape[1] // head_dim
    group_size = head_count // key_heads
    token_rows = tokens.reshape(seq_count * seq_length, model_width)
    query_rows = jnp.dot(token_rows, query_weight, preferred_element_type=jnp.float32).astype(jnp.bfloat16)
    query_rows = query_rows.reshape(seq_count, seq_length, head_count, head_dim)
    key_rows = jnp.dot(token_rows, key_weight, preferred_element_type=jnp.float32).astype(jnp.bfloat16)
    key_rows = key_rows.reshape(seq_count, seq_length, key_heads, head_dim)
    value_rows = jnp.dot(token_rows, value_weight, preferred_element_type=jnp.float32).astype(jnp.bfloat16)
    value_rows = value_rows.reshape(seq_count, seq_length, key_heads, head_dim)
    gate_input = jnp.dot(token_rows, forget_weight, preferred_element_type=jnp.float32) + forget_bias[None, :]
    log_gate = jax.nn.log_sigmoid(gate_input).astype(jnp.bfloat16).reshape(seq_count, seq_length, head_count)
    decay_sum = jnp.cumsum(log_gate.astype(jnp.float32), axis=1)
    block_size = pick_block(seq_length)
    block_count = seq_length // block_size
    score_scale = head_dim ** -0.5
    positions = jnp.arange(seq_length, dtype=jnp.int32)
    offsets = jnp.arange(block_size, dtype=jnp.int32)

    def one_block(flat_index):
        seq_index = flat_index // (head_count * block_count)
        head_index = (flat_index // block_count) % head_count
        block_index = flat_index % block_count
        first_row = block_index * block_size
        zero_index = jnp.zeros((), jnp.int32)
        key_index = head_index // group_size
        query_part = lax.dynamic_slice(query_rows, (seq_index, first_row, head_index, zero_index),
                                       (1, block_size, 1, head_dim)).reshape(block_size, head_dim)
        key_part = lax.dynamic_slice(key_rows, (seq_index, zero_index, key_index, zero_index),
                                     (1, seq_length, 1, head_dim)).reshape(seq_length, head_dim)
        value_part = lax.dynamic_slice(value_rows, (seq_index, zero_index, key_index, zero_index),
                                       (1, seq_length, 1, head_dim)).reshape(seq_length, head_dim)
        decay_row = lax.dynamic_slice(decay_sum, (seq_index, zero_index, head_index),
                                      (1, seq_length, 1)).reshape(seq_length)
        query_decay = lax.dynamic_slice_in_dim(decay_row, first_row, block_size)
        raw_scores = jnp.dot(query_part, key_part.T, preferred_element_type=jnp.float32)
        biased = raw_scores * score_scale + query_decay[:, None] - decay_row[None, :]
        allowed = positions[None, :] <= (first_row + offsets)[:, None]
        masked = jnp.where(allowed, biased, -jnp.inf)
        shifted = jnp.exp(masked - jnp.max(masked, axis=-1, keepdims=True))
        weights = (shifted / jnp.sum(shifted, axis=-1, keepdims=True)).astype(jnp.bfloat16)
        return jnp.dot(weights, value_part, preferred_element_type=jnp.float32).astype(jnp.bfloat16)

    flat_blocks = lax.map(one_block, jnp.arange(seq_count * head_count * block_count, dtype=jnp.int32))
    flat_blocks = flat_blocks.reshape(seq_count, head_count, block_count, block_size, head_dim)
    return flat_blocks.transpose(0, 2, 3, 1, 4).reshape(seq_count, seq_length, head_count * head_dim)
```

```python
import functools
import math

import jax
import jax.numpy as jnp
from jax import lax
from jax.experimental import pallas as pl
from jax.experimental.pallas import tpu as pltpu
from jax.sharding import PartitionSpec as P

BF16 = jnp.bfloat16
F32 = jnp.float32
MESH = pl.DeviceIdType.MESH
SIDE = 4
KEYS, VALUES, GATES = 0, 1, 2
UP, DOWN = 0, 1
NT = (((1,), (1,)), ((), ()))
TN = (((0,), (0,)), ((), ()))

WHOLE = [("W", 1, 0), ("W", 3, 0), ("W", 0, 1), ("W", 0, 3), ("W", 2, 0), ("W", 0, 2)]
HALVES = [(part, a, b) for part in "AB" for a in (1, 2, 3) for b in (1, 2, 3)]
ITEM = {key: n for n, key in enumerate(WHOLE + HALVES)}


class Gather:
    def __init__(self, number, shard, full, local_sem, sends, receives, pair_sends, pair_receives, place):
        self.number, self.shard, self.full, self.local_sem = number, shard, full, local_sem
        self.sems = (sends, receives, pair_sends, pair_receives)
        self.place = place
        self.depth = shard.shape[0]
        self.started = []

    def slot(self, a, b, other=False):
        x, y, core, turn = self.place
        if other:
            core, turn = 1 - core, -turn
        across = lax.rem(x + turn * a + 2 * SIDE, SIDE)
        along = lax.rem(y + turn * b + 2 * SIDE, SIDE)
        return (along * SIDE + across) * 2 + core

    def rows(self, key, other=False):
        part, a, b = key
        first = self.slot(a, b, other) * self.depth
        count = self.depth if part == "W" else self.depth // 2
        if part == "B":
            first = first + count
        return self.full.at[pl.ds(pl.multiple_of(first, count), count)]

    def copy(self, key, received, target):
        sends, receives = self.sems[:2]
        n = ITEM[received]
        view = self.rows(key)
        return pltpu.make_async_remote_copy(
            src_ref=view,
            dst_ref=view,
            send_sem=sends.at[self.number, n],
            recv_sem=receives.at[self.number, n],
            device_id={"dp": target},
            device_id_type=MESH,
        )

    def send(self, key, dx, dy):
        part, a, b = key
        received = (part, (a - dx) % SIDE, (b - dy) % SIDE)
        copy = self.copy(key, received, self.slot(dx, dy))
        copy.start()
        self.started.append(copy)

    def wait(self, key):
        self.copy(key, key, self.slot(1, 0)).wait_recv()

    def pair_copy(self, a, b, other=False):
        x, y, core, turn = self.place
        view = self.rows(("W", a, b), other)
        return pltpu.make_async_remote_copy(
            src_ref=view,
            dst_ref=view,
            send_sem=self.sems[2].at[self.number, a * SIDE + b],
            recv_sem=self.sems[3].at[self.number, a * SIDE + b],
            device_id={"dp": (y * SIDE + x) * 2 + 1 - core},
            device_id_type=MESH,
        )

    def share(self, a, b):
        copy = self.pair_copy(a, b)
        copy.start()
        self.started.append(copy)

    def fetch(self):
        self.fetched = pltpu.make_async_copy(self.shard, self.rows(("W", 0, 0)), self.local_sem.at[self.number])
        self.fetched.start()

    def begin(self):
        self.fetched.wait()
        for dx, dy in ((1, 0), (0, 1), (-1, 0), (0, -1)):
            self.send(("W", 0, 0), dx, dy)
        self.share(0, 0)

    def first(self):
        for a in (3, 1):
            self.wait(("W", a, 0))
            if a == 3:
                self.send(("W", 3, 0), 1, 0)
            for dy in (1, -1):
                self.send(("A", a, 0), 0, dy)
            self.wait(("W", 0, a))
            if a == 3:
                self.send(("W", 0, 3), 0, 1)
            for dx in (1, -1):
                self.send(("B", 0, a), dx, 0)
            self.share(a, 0)
            self.share(0, a)

    def second(self):
        for a in (3, 1):
            self.wait(("A", a, 3))
            self.send(("A", a, 3), 0, 1)
            self.wait(("B", 3, a))
            self.send(("B", 3, a), 1, 0)
        self.wait(("W", 2, 0))
        for dy in (1, -1):
            self.send(("A", 2, 0), 0, dy)
        self.wait(("W", 0, 2))
        for dx in (1, -1):
            self.send(("B", 0, 2), dx, 0)
        self.share(2, 0)
        self.share(0, 2)
        for a in (3, 1):
            self.wait(("A", a, 1))
            self.wait(("B", 1, a))
        for a in (3, 1):
            for b in (3, 1):
                self.share(a, b)

    def third(self):
        self.wait(("A", 2, 3))
        self.send(("A", 2, 3), 0, 1)
        self.wait(("B", 3, 2))
        self.send(("B", 3, 2), 1, 0)
        for a in (3, 1):
            self.wait(("A", a, 2))
            self.wait(("B", 2, a))
        self.wait(("A", 2, 1))
        self.wait(("B", 1, 2))
        for a in (3, 1):
            self.share(2, a)
            self.share(a, 2)

    def fourth(self):
        self.wait(("A", 2, 2))
        self.wait(("B", 2, 2))
        self.share(2, 2)

    def complete(self):
        for a in range(SIDE):
            for b in range(SIDE):
                self.pair_copy(a, b, other=True).wait_recv()

    def drain(self):
        for copy in self.started:
            copy.wait_send()


def kernel(
    tokens, query_shard, key_shard, value_shard, forget_weight, forget_bias, out,
    query_all, key_all, value_all, keys, values, gates, key_extra, queries, totals, peaks, sums,
    local_sem, sends, receives, pair_sends, pair_receives, ring_sends, ring_receives,
):
    ring = lax.axis_size("sp")
    half = ring // 2
    me = lax.axis_index("sp")
    mine = lax.axis_index("dp")
    core = lax.rem(mine, 2)
    x = lax.rem(lax.div(mine, 2), SIDE)
    y = lax.div(mine, 2 * SIDE)
    place = (x, y, core, 1 - 2 * core)
    rows = tokens.shape[0]
    heads = forget_weight.shape[1]
    groups, dim = keys.shape[1], keys.shape[3]
    share = heads // groups
    root = math.sqrt(dim)

    gather_keys, gather_values, gather_queries = (
        Gather(n, shard, full, local_sem, sends, receives, pair_sends, pair_receives, place)
        for n, (shard, full) in enumerate(
            ((key_shard, key_all), (value_shard, value_all), (query_shard, query_all))
        )
    )
    for g in (gather_keys, gather_values, gather_queries):
        g.fetch()

    above, below = lax.rem(me + 1, ring), lax.rem(me + ring - 1, ring)
    barrier = pltpu.get_barrier_semaphore()
    for dx, dy in ((1, 0), (0, 1), (-1, 0), (0, -1)):
        pl.semaphore_signal(
            barrier, inc=1, device_id={"dp": gather_keys.slot(dx, dy)}, device_id_type=MESH
        )
    pl.semaphore_signal(barrier, inc=1, device_id={"dp": mine + 1 - 2 * core}, device_id_type=MESH)
    for neighbour in (above, below):
        pl.semaphore_signal(barrier, inc=1, device_id={"sp": neighbour}, device_id_type=MESH)
    pl.semaphore_wait(barrier, 7)

    buffers = {KEYS: keys, VALUES: values, GATES: gates}
    last = {
        (KEYS, UP): half, (KEYS, DOWN): half - 1,
        (VALUES, UP): half - 1, (VALUES, DOWN): half,
        (GATES, UP): half, (GATES, DOWN): half - 1,
    }

    def hop(kind, way, step, slot):
        view = buffers[kind].at[slot]
        return pltpu.make_async_remote_copy(
            src_ref=view,
            dst_ref=view,
            send_sem=ring_sends.at[kind, way, step - 1],
            recv_sem=ring_receives.at[kind, way, step - 1],
            device_id={"sp": above if way == UP else below},
            device_id_type=MESH,
        )

    def origin(way, step):
        return lax.rem(me - step + ring, ring) if way == UP else lax.rem(me + step, ring)

    def launch(kind):
        for way in (UP, DOWN):
            hop(kind, way, 1, me).start()

    def relay(kind, step):
        for way in (UP, DOWN):
            final = last[kind, way]
            slot = origin(way, step)
            if isinstance(step, int):
                if step <= final:
                    hop(kind, way, step, slot).wait_recv()
                if step < final:
                    hop(kind, way, step + 1, slot).start()
            else:
                hop(kind, way, step, slot).wait_recv()

                @pl.when(step < final)
                def _():
                    hop(kind, way, step + 1, slot).start()

    gather_keys.begin()
    gather_values.begin()

    wide = gates.shape[2]
    gate_input = jnp.dot(tokens[...], forget_weight[...], preferred_element_type=F32) + forget_bias[...]
    log_gate = (jnp.minimum(gate_input, 0.0) - jnp.log1p(jnp.exp(-jnp.abs(gate_input)))).astype(BF16)
    eye = (
        lax.broadcasted_iota(jnp.int32, (rows, wide), 0) == lax.broadcasted_iota(jnp.int32, (rows, wide), 1)
    ).astype(F32).astype(BF16)
    gates[me] = lax.dot_general(log_gate, eye, TN, preferred_element_type=F32).astype(BF16)

    gather_keys.first()
    launch(GATES)
    gather_values.first()
    relay(GATES, 1)
    gather_keys.second()
    relay(GATES, 2)
    gather_values.second()
    gather_keys.third()
    relay(GATES, 3)
    gather_queries.begin()
    gather_keys.fourth()
    relay(GATES, 4)
    gather_keys.complete()

    def project(weight, block):
        def one(g, carry):
            columns = pl.ds(pl.multiple_of(g * dim * 2, dim * 2), dim * 2)
            part = jnp.dot(tokens[...], weight[:, columns], preferred_element_type=F32).astype(BF16)
            block[me, 2 * g] = part[:, :dim]
            block[me, 2 * g + 1] = part[:, dim:]
            return carry

        lax.fori_loop(0, groups // 2, one, 0)

    project(key_all, keys)
    gather_values.third()
    launch(KEYS)
    relay(GATES, 5)
    gather_values.fourth()
    gather_values.complete()
    project(value_all, values)
    relay(GATES, 6)
    launch(VALUES)
    gather_queries.first()
    relay(GATES, 7)
    relay(GATES, 8)

    lane = lax.broadcasted_iota(jnp.int32, (rows, dim), 1)
    tall = rows + 8
    down = lax.broadcasted_iota(jnp.int32, (tall, wide), 0)
    right = lax.broadcasted_iota(jnp.int32, (tall, wide), 1)
    later = ((right > down) | (down >= rows)).astype(F32).astype(BF16)
    sofar = ((right <= down) & (down < rows)).astype(F32).astype(BF16)

    def thrice(block):
        g = gates[block]
        return jnp.concatenate([g, g, g, jnp.zeros((dim - 3 * heads, wide), BF16)], axis=0)

    def parts(exact):
        hi = exact.astype(BF16).astype(F32)
        rest = exact - hi
        mid = rest.astype(BF16).astype(F32)
        low = rest - mid
        return jnp.where(
            lane < heads, hi, jnp.where(lane < 2 * heads, mid, jnp.where(lane < 3 * heads, low, 0.0))
        )

    ones = ((lane >= 3 * heads) & (lane < 3 * heads + 3)).astype(F32)

    def decay_of(step, after):
        block = lax.rem(me - step + ring, ring)
        summed = lax.dot_general(later, thrice(block), NT, preferred_element_type=F32)
        key_extra[block] = (parts((summed[:rows] + after) * root) + ones).astype(BF16)
        return after + summed[rows : rows + 1]

    own = lax.dot_general(later, thrice(me), NT, preferred_element_type=F32)[rows : rows + 1]
    lax.fori_loop(0, ring, decay_of, -own)

    own_sum = lax.dot_general(sofar, thrice(me), NT, preferred_element_type=F32)[:rows]
    own_parts = parts(own_sum * root).astype(BF16)
    pick_row = lax.broadcasted_iota(jnp.int32, (dim, dim), 0)
    pick_lane = lax.broadcasted_iota(jnp.int32, (dim, dim), 1)

    def query_extra(h, carry):
        pick = ((pick_row == h + heads * (pick_lane - 3 * heads)) & (pick_lane >= 3 * heads)
                & (pick_lane < 3 * heads + 3)).astype(F32).astype(BF16)
        moved = jnp.dot(own_parts, pick, preferred_element_type=F32)
        hot = ((lane == h) | (lane == h + heads) | (lane == h + 2 * heads)).astype(F32)
        place_rows = pl.ds(pl.multiple_of(lax.rem(h, share) * rows, rows), rows)
        queries[lax.div(h, share), place_rows, dim:] = (moved + hot).astype(BF16)
        return carry

    lax.fori_loop(0, heads, query_extra, 0)

    relay(KEYS, 1)
    relay(VALUES, 1)
    gather_queries.second()
    relay(KEYS, 2)
    relay(VALUES, 2)
    gather_queries.third()
    relay(KEYS, 3)
    gather_queries.fourth()
    relay(VALUES, 3)
    gather_queries.complete()

    def query_group(g, carry):
        columns = pl.ds(pl.multiple_of(g * dim * share, dim * share), dim * share)
        part = jnp.dot(tokens[...], query_all[:, columns], preferred_element_type=F32).astype(BF16)
        for h in range(share):
            queries[g, h * rows : (h + 1) * rows, :dim] = part[:, h * dim : (h + 1) * dim]
        return carry

    lax.fori_loop(0, groups, query_group, 0)

    scale = 1.0 / root
    breadth = share * rows

    def attend(block, diagonal=False):
        def one(g, carry):
            key_part = jnp.concatenate([keys[block, g], key_extra[block]], axis=1)
            score = lax.dot_general(key_part, queries[g], NT, preferred_element_type=F32) * scale
            if diagonal:
                key_at = lax.broadcasted_iota(jnp.int32, (rows, breadth), 0)
                query_at = lax.broadcasted_iota(jnp.int32, (rows, breadth), 1)
                for h in range(share - 1, 0, -1):
                    query_at = jnp.where(query_at >= h * rows, query_at - h * rows, query_at)
                score = jnp.where(key_at <= query_at, score, -jnp.inf)
                peak = jnp.max(score, axis=0, keepdims=True)
            else:
                old = peaks[g]
                peak = jnp.maximum(old, jnp.max(score, axis=0, keepdims=True))
            weight = jnp.exp(score - peak)
            total = jnp.sum(weight, axis=0, keepdims=True)
            mixed = lax.dot_general(values[block, g], weight.astype(BF16), TN, preferred_element_type=F32)
            peaks[g] = peak
            if diagonal:
                sums[g] = total
                totals[g] = mixed
            else:
                fade = jnp.exp(old - peak)
                sums[g] = sums[g] * fade + total
                totals[g] = totals[g] * fade + mixed
            return carry

        lax.fori_loop(0, groups, one, 0)

    def unit(u):
        step = lax.div(u, 2) + 1
        upward = lax.rem(u, 2) == 0
        block = jnp.where(upward, me - step, me + step - ring)

        @pl.when(block >= 0)
        def _():
            attend(block)

    attend(me, diagonal=True)

    def steady(step, carry):
        relay(KEYS, step)
        unit(3 * (step - 4))
        unit(3 * (step - 4) + 1)
        relay(VALUES, step)
        unit(3 * (step - 4) + 2)
        return carry

    lax.fori_loop(4, half, steady, 0)
    relay(KEYS, half)
    for u in range(3 * (half - 4), 2 * (half - 1)):
        unit(u)
    relay(VALUES, half)

    @pl.when(me >= half)
    def _():
        attend(me - half)

    for g in range(groups):
        mixed = (totals[g] / sums[g]).T
        for h in range(share):
            at = (g * share + h) * dim
            out[:, at : at + dim] = mixed[h * rows : (h + 1) * rows].astype(BF16)

    for g in (gather_keys, gather_values, gather_queries):
        g.drain()
    for kind in (KEYS, VALUES, GATES):
        for way in (UP, DOWN):
            def sent(n, carry, kind=kind, way=way):
                hop(kind, way, n + 1, me).wait_send()
                return carry

            lax.fori_loop(0, last[kind, way], sent, 0)


def on_device(tokens, query_weight, key_weight, value_weight, forget_weight, forget_bias):
    token_rows = tokens[0]
    rows, width = token_rows.shape
    ring = lax.axis_size("sp")
    heads = forget_weight.shape[1]
    dim = query_weight.shape[1] // heads
    groups = key_weight.shape[1] // dim
    share = heads // groups
    wide = -(-rows // 128) * 128
    vmem = pl.BlockSpec(memory_space=pltpu.VMEM)
    anywhere = pl.BlockSpec(memory_space=pl.ANY)
    mixed = pl.pallas_call(
        kernel,
        out_shape=jax.ShapeDtypeStruct((rows, heads * dim), BF16),
        in_specs=[vmem, anywhere, anywhere, anywhere, vmem, vmem],
        out_specs=vmem,
        scratch_shapes=[
            pltpu.VMEM((width, heads * dim), BF16),
            pltpu.VMEM((width, groups * dim), BF16),
            pltpu.VMEM((width, groups * dim), BF16),
            pltpu.VMEM((ring, groups, rows, dim), BF16),
            pltpu.VMEM((ring, groups, rows, dim), BF16),
            pltpu.VMEM((ring, heads, wide), BF16),
            pltpu.VMEM((ring, rows, dim), BF16),
            pltpu.VMEM((groups, share * rows, 2 * dim), BF16),
            pltpu.VMEM((groups, dim, share * rows), F32),
            pltpu.VMEM((groups, 1, share * rows), F32),
            pltpu.VMEM((groups, 1, share * rows), F32),
            pltpu.SemaphoreType.DMA((3,)),
            pltpu.SemaphoreType.DMA((3, len(ITEM))),
            pltpu.SemaphoreType.DMA((3, len(ITEM))),
            pltpu.SemaphoreType.DMA((3, SIDE * SIDE)),
            pltpu.SemaphoreType.DMA((3, SIDE * SIDE)),
            pltpu.SemaphoreType.DMA((3, 2, ring // 2)),
            pltpu.SemaphoreType.DMA((3, 2, ring // 2)),
        ],
        compiler_params=pltpu.CompilerParams(
            collective_id=0, has_side_effects=True, vmem_limit_bytes=60 * 2**20
        ),
    )(token_rows, query_weight, key_weight, value_weight, forget_weight, forget_bias[None, :])
    return mixed[None]


def solution(mesh):
    placed = (P("dp", "sp", None), P("dp", None), P("dp", None), P("dp", None), P(), P())
    return jax.shard_map(
        on_device, mesh=mesh, in_specs=placed, out_specs=P("dp", "sp", None), check_vma=False
    )
```

```python
import functools
import math

import jax
import jax.numpy as jnp
from jax import lax
from jax.experimental import pallas as pl
from jax.experimental.pallas import tpu as pltpu
from jax.sharding import PartitionSpec as P

BF16 = jnp.bfloat16
F32 = jnp.float32
MESH = pl.DeviceIdType.MESH
SIDE = 4
KEYS, VALUES, GATES = 0, 1, 2
UP, DOWN = 0, 1
NT = (((1,), (1,)), ((), ()))
TN = (((0,), (0,)), ((), ()))

WHOLE = [("W", 1, 0), ("W", 3, 0), ("W", 0, 1), ("W", 0, 3), ("W", 2, 0), ("W", 0, 2)]
HALVES = [(part, a, b) for part in "AB" for a in (1, 2, 3) for b in (1, 2, 3)]
OWN = ("W", 0, 0)
ITEM = {key: n for n, key in enumerate(WHOLE + HALVES)}


def copy_rows(part, depth):
    return depth if part == "W" else depth // 2


class Gather:
    def __init__(self, number, shard, full, sends, receives, pair_sends, pair_receives, place):
        self.number, self.shard, self.full = number, shard, full
        self.sems = (sends, receives, pair_sends, pair_receives)
        self.place = place
        self.depth = shard.shape[0]
        self.sent = 0

    def slot(self, a, b, other=False):
        x, y, core, turn = self.place
        if other:
            core, turn = 1 - core, -turn
        across = lax.rem(x + turn * a + 2 * SIDE, SIDE)
        along = lax.rem(y + turn * b + 2 * SIDE, SIDE)
        return (along * SIDE + across) * 2 + core

    def rows(self, key, other=False):
        part, a, b = key
        first = self.slot(a, b, other) * self.depth
        count = copy_rows(part, self.depth)
        if part == "B":
            first = first + count
        return self.full.at[pl.ds(pl.multiple_of(first, count), count)]

    def copy(self, key, received, target):
        sends, receives = self.sems[:2]
        n = ITEM[received]
        view = self.rows(key)
        return pltpu.make_async_remote_copy(
            src_ref=self.shard if key == OWN else view,
            dst_ref=view,
            send_sem=sends.at[self.number],
            recv_sem=receives.at[self.number, n],
            device_id={"dp": target},
            device_id_type=MESH,
        )

    def send(self, key, dx, dy):
        part, a, b = key
        received = (part, (a - dx) % SIDE, (b - dy) % SIDE)
        copy = self.copy(key, received, self.slot(dx, dy))
        copy.start()
        self.sent += copy_rows(part, self.depth)

    def wait(self, key):
        self.copy(key, key, self.slot(1, 0)).wait_recv()

    def pair_copy(self, a, b, other=False):
        x, y, core, turn = self.place
        view = self.rows(("W", a, b), other)
        return pltpu.make_async_remote_copy(
            src_ref=view if a or b or other else self.shard,
            dst_ref=view,
            send_sem=self.sems[2].at[self.number],
            recv_sem=self.sems[3].at[self.number],
            device_id={"dp": (y * SIDE + x) * 2 + 1 - core},
            device_id_type=MESH,
        )

    def share(self, a, b):
        self.pair_copy(a, b).start()

    def begin(self):
        for dx, dy in ((1, 0), (0, 1), (-1, 0), (0, -1)):
            self.send(OWN, dx, dy)
        self.share(0, 0)
        self.rows(OWN)[...] = self.shard[...]

    def first(self):
        for a in (3, 1):
            self.wait(("W", a, 0))
            if a == 3:
                self.send(("W", 3, 0), 1, 0)
            for dy in (1, -1):
                self.send(("A", a, 0), 0, dy)
            self.wait(("W", 0, a))
            if a == 3:
                self.send(("W", 0, 3), 0, 1)
            for dx in (1, -1):
                self.send(("B", 0, a), dx, 0)
            self.share(a, 0)
            self.share(0, a)

    def second(self):
        for a in (3, 1):
            self.wait(("A", a, 3))
            self.send(("A", a, 3), 0, 1)
            self.wait(("B", 3, a))
            self.send(("B", 3, a), 1, 0)
        self.wait(("W", 2, 0))
        for dy in (1, -1):
            self.send(("A", 2, 0), 0, dy)
        self.wait(("W", 0, 2))
        for dx in (1, -1):
            self.send(("B", 0, 2), dx, 0)
        self.share(2, 0)
        self.share(0, 2)
        for a in (3, 1):
            self.wait(("A", a, 1))
            self.wait(("B", 1, a))
        for a in (3, 1):
            for b in (3, 1):
                self.share(a, b)

    def third(self):
        self.wait(("A", 2, 3))
        self.send(("A", 2, 3), 0, 1)
        self.wait(("B", 3, 2))
        self.send(("B", 3, 2), 1, 0)
        for a in (3, 1):
            self.wait(("A", a, 2))
            self.wait(("B", 2, a))
        self.wait(("A", 2, 1))
        self.wait(("B", 1, 2))
        for a in (3, 1):
            self.share(2, a)
            self.share(a, 2)

    def fourth(self):
        self.wait(("A", 2, 2))
        self.wait(("B", 2, 2))
        self.share(2, 2)

    def bulk(self, rows, send_sem, receive_sem):
        view = self.full.at[pl.ds(0, rows)]
        return pltpu.make_async_remote_copy(
            src_ref=view,
            dst_ref=view,
            send_sem=send_sem.at[self.number],
            recv_sem=receive_sem.at[self.number],
            device_id={"dp": self.slot(1, 0)},
            device_id_type=MESH,
        )

    def complete(self):
        self.bulk(SIDE * SIDE * self.depth, self.sems[2], self.sems[3]).wait_recv()

    def drain(self):
        self.bulk(self.sent, self.sems[0], self.sems[3]).wait_send()
        self.bulk(SIDE * SIDE * self.depth, self.sems[2], self.sems[3]).wait_send()


def kernel(
    tokens, query_shard, key_shard, value_shard, forget_weight, forget_bias, out,
    near, query_all, key_all, value_all, keys, values, gates, key_extra, queries, totals, peaks, sums,
    sends, receives, pair_sends, pair_receives, ring_sends, ring_receives, near_sends, near_receives,
):
    ring = lax.axis_size("sp")
    half = ring // 2
    me = lax.axis_index("sp")
    mine = lax.axis_index("dp")
    core = lax.rem(mine, 2)
    x = lax.rem(lax.div(mine, 2), SIDE)
    y = lax.div(mine, 2 * SIDE)
    place = (x, y, core, 1 - 2 * core)
    rows = tokens.shape[0]
    heads = forget_weight.shape[0]
    groups, dim = keys.shape[1], keys.shape[3]
    share = heads // groups
    root = math.sqrt(dim)

    gather_keys, gather_values, gather_queries = (
        Gather(n, shard, full, sends, receives, pair_sends, pair_receives, place)
        for n, (shard, full) in enumerate(
            ((key_shard, key_all), (value_shard, value_all), (query_shard, query_all))
        )
    )

    above, below = lax.rem(me + 1, ring), lax.rem(me + ring - 1, ring)
    barrier = pltpu.get_barrier_semaphore()
    for dx, dy in ((1, 0), (0, 1), (-1, 0), (0, -1)):
        pl.semaphore_signal(
            barrier, inc=1, device_id={"dp": gather_keys.slot(dx, dy)}, device_id_type=MESH
        )
    pl.semaphore_signal(barrier, inc=1, device_id={"dp": mine + 1 - 2 * core}, device_id_type=MESH)
    for neighbour in (above, below):
        pl.semaphore_signal(barrier, inc=1, device_id={"sp": neighbour}, device_id_type=MESH)
    pl.semaphore_wait(barrier, 7)

    buffers = {KEYS: keys, VALUES: values, GATES: gates}
    last = {
        (KEYS, UP): half, (KEYS, DOWN): half - 1,
        (VALUES, UP): half - 1, (VALUES, DOWN): half,
        (GATES, UP): half, (GATES, DOWN): half - 1,
    }

    def hop(kind, way, step, slot):
        view = buffers[kind].at[slot]
        return pltpu.make_async_remote_copy(
            src_ref=view,
            dst_ref=view,
            send_sem=ring_sends.at[kind, way, step - 1],
            recv_sem=ring_receives.at[kind, way, step - 1],
            device_id={"sp": above if way == UP else below},
            device_id_type=MESH,
        )

    def origin(way, step):
        return lax.rem(me - step + ring, ring) if way == UP else lax.rem(me + step, ring)

    def launch(kind, way):
        hop(kind, way, 2, origin(way, 1)).start()

    def relay(kind, step):
        for way in (UP, DOWN):
            final = last[kind, way]
            slot = origin(way, step)
            if isinstance(step, int):
                if step <= final:
                    hop(kind, way, step, slot).wait_recv()
                if step < final:
                    hop(kind, way, step + 1, slot).start()
                if 3 <= step <= final:
                    hop(kind, way, step - 1, slot).wait_send()
            else:
                hop(kind, way, step, slot).wait_recv()

                @pl.when(step < final)
                def _():
                    hop(kind, way, step + 1, slot).start()

                hop(kind, way, step - 1, slot).wait_send()

    def visit(way):
        return pltpu.make_async_remote_copy(
            src_ref=tokens,
            dst_ref=near.at[way],
            send_sem=near_sends.at[way],
            recv_sem=near_receives.at[way],
            device_id={"sp": above if way == UP else below},
            device_id_type=MESH,
        )

    wide = gates.shape[2]
    bias_at = lax.broadcasted_iota(jnp.int32, (heads, heads), 0) == lax.broadcasted_iota(jnp.int32, (heads, heads), 1)
    bias = jnp.sum(jnp.where(bias_at, forget_bias[...], 0.0), axis=1, keepdims=True)
    eye = (
        lax.broadcasted_iota(jnp.int32, (rows, wide), 0) == lax.broadcasted_iota(jnp.int32, (rows, wide), 1)
    ).astype(F32).astype(BF16)

    def gate(source, block):
        gate_input = lax.dot_general(forget_weight[...], source[...], NT, preferred_element_type=F32) + bias
        log_gate = (jnp.minimum(gate_input, 0.0) - jnp.log1p(jnp.exp(-jnp.abs(gate_input)))).astype(BF16)
        gates[block] = jnp.dot(log_gate, eye, preferred_element_type=F32).astype(BF16)

    def project(source, weight, buffer, block):
        def one(g, carry):
            columns = pl.ds(pl.multiple_of(g * dim * 2, dim * 2), dim * 2)
            part = jnp.dot(source[...], weight[:, columns], preferred_element_type=F32).astype(BF16)
            buffer[block, 2 * g] = part[:, :dim]
            buffer[block, 2 * g + 1] = part[:, dim:]
            return carry

        lax.fori_loop(0, groups // 2, one, 0)

    lane = lax.broadcasted_iota(jnp.int32, (rows, dim), 1)
    tall = rows + 8
    down = lax.broadcasted_iota(jnp.int32, (tall, wide), 0)
    right = lax.broadcasted_iota(jnp.int32, (tall, wide), 1)
    later = ((right > down) | (down >= rows)).astype(F32).astype(BF16)
    sofar = ((right <= down) & (down < rows)).astype(F32).astype(BF16)

    def thrice(block):
        g = gates[block]
        return jnp.concatenate([g, g, g, jnp.zeros((dim - 3 * heads, wide), BF16)], axis=0)

    def parts(exact):
        hi = exact.astype(BF16).astype(F32)
        rest = exact - hi
        mid = rest.astype(BF16).astype(F32)
        low = rest - mid
        return jnp.where(
            lane < heads, hi, jnp.where(lane < 2 * heads, mid, jnp.where(lane < 3 * heads, low, 0.0))
        )

    ones = ((lane >= 3 * heads) & (lane < 3 * heads + 3)).astype(F32)

    def decay_of(step, after):
        block = lax.rem(me - step + ring, ring)
        summed = lax.dot_general(later, thrice(block), NT, preferred_element_type=F32)
        key_extra[block] = (parts((summed[:rows] + after) * root) + ones).astype(BF16)
        return after + summed[rows : rows + 1]

    def decays():
        own = lax.dot_general(later, thrice(me), NT, preferred_element_type=F32)[rows : rows + 1]
        lax.fori_loop(0, ring, decay_of, -own)

    def query_extras(first, end):
        own_sum = lax.dot_general(sofar, thrice(me), NT, preferred_element_type=F32)[:rows]
        own_parts = parts(own_sum * root).astype(BF16)
        pick_row = lax.broadcasted_iota(jnp.int32, (dim, dim), 0)
        pick_lane = lax.broadcasted_iota(jnp.int32, (dim, dim), 1)

        def query_extra(h, carry):
            pick = ((pick_row == h + heads * (pick_lane - 3 * heads)) & (pick_lane >= 3 * heads)
                    & (pick_lane < 3 * heads + 3)).astype(F32).astype(BF16)
            moved = jnp.dot(own_parts, pick, preferred_element_type=F32)
            hot = ((lane == h) | (lane == h + heads) | (lane == h + 2 * heads)).astype(F32)
            place_rows = pl.ds(pl.multiple_of(lax.rem(h, share) * rows, rows), rows)
            queries[lax.div(h, share), place_rows, dim:] = (moved + hot).astype(BF16)
            return carry

        lax.fori_loop(first, end, query_extra, 0)

    def query_group(g, carry):
        columns = pl.ds(pl.multiple_of(g * dim * share, dim * share), dim * share)
        part = jnp.dot(tokens[...], query_all[:, columns], preferred_element_type=F32).astype(BF16)
        for h in range(share):
            queries[g, h * rows : (h + 1) * rows, :dim] = part[:, h * dim : (h + 1) * dim]
        return carry

    scale = math.log2(math.e) / root
    breadth = share * rows

    def attend(blocks, some_groups, diagonal=False):
        key_rows = rows * len(blocks)
        for g in some_groups:
            key_part = jnp.concatenate(
                [jnp.concatenate([keys[block, g], key_extra[block]], axis=1) for block in blocks], axis=0
            )
            value_part = jnp.concatenate([values[block, g] for block in blocks], axis=0)
            score = lax.dot_general(key_part, queries[g], NT, preferred_element_type=F32)
            if diagonal:
                key_at = lax.broadcasted_iota(jnp.int32, (key_rows, breadth), 0)
                query_at = lax.broadcasted_iota(jnp.int32, (key_rows, breadth), 1)
                for h in range(share - 1, 0, -1):
                    query_at = jnp.where(query_at >= h * rows, query_at - h * rows, query_at)
                score = jnp.where(key_at <= query_at, score, -jnp.inf)
                peak = jnp.max(score, axis=0, keepdims=True)
            else:
                old = peaks[g]
                peak = jnp.maximum(old, jnp.max(score, axis=0, keepdims=True))
            weight = jnp.exp2((score - peak) * scale)
            total = jnp.sum(weight, axis=0, keepdims=True)
            mixed = lax.dot_general(value_part, weight.astype(BF16), TN, preferred_element_type=F32)
            peaks[g] = peak
            if diagonal:
                sums[g] = total
                totals[g] = mixed
            else:
                fade = jnp.exp2((old - peak) * scale)
                sums[g] = sums[g] * fade + total
                totals[g] = totals[g] * fade + mixed

    def attend_own(n, carry):
        attend((me,), (2 * n, 2 * n + 1), diagonal=True)
        return carry

    def unit(u, carry):
        step = lax.div(u, 2) + 1
        some = (2 * lax.rem(u, 2), 2 * lax.rem(u, 2) + 1)
        low, high = me - step, me + step - ring

        @pl.when((low >= 0) & (high >= 0))
        def _():
            attend((low, high), some)

        @pl.when(((low >= 0) | (high >= 0)) & ((low < 0) | (high < 0)))
        def _():
            attend((jnp.maximum(low, high),), some)

        return carry

    gather_keys.begin()
    for way in (UP, DOWN):
        visit(way).start()
    gate(tokens, me)
    gather_keys.first()
    gather_values.begin()
    gather_keys.second()
    gather_values.first()
    gather_keys.third()
    gather_values.second()
    gather_queries.begin()
    gather_keys.fourth()
    gather_keys.complete()
    project(tokens, key_all, keys, me)
    gather_values.third()
    visit(UP).wait_recv()
    gate(near.at[UP], below)
    project(near.at[UP], key_all, keys, below)
    visit(DOWN).wait_recv()
    gate(near.at[DOWN], above)
    launch(GATES, UP)
    launch(KEYS, UP)
    project(near.at[DOWN], key_all, keys, above)
    gather_queries.first()
    launch(GATES, DOWN)
    launch(KEYS, DOWN)
    gather_values.fourth()
    gather_values.complete()
    project(near.at[UP], value_all, values, below)
    project(near.at[DOWN], value_all, values, above)
    relay(GATES, 2)
    launch(VALUES, UP)
    project(tokens, value_all, values, me)
    launch(VALUES, DOWN)
    query_extras(0, heads)
    relay(GATES, 3)
    relay(KEYS, 2)
    gather_queries.second()
    relay(GATES, 4)
    relay(VALUES, 2)
    gather_keys.drain()
    gather_values.drain()
    relay(GATES, 5)
    relay(KEYS, 3)
    gather_queries.third()
    relay(GATES, 6)
    relay(VALUES, 3)
    gather_queries.fourth()
    relay(GATES, 7)
    relay(KEYS, 4)
    for way in (UP, DOWN):
        visit(way).wait_send()
    gather_queries.complete()
    lax.fori_loop(0, groups, query_group, 0)
    relay(GATES, 8)
    relay(VALUES, 4)
    decays()
    lax.fori_loop(0, groups // 2, attend_own, 0)

    def steady(step, carry):
        done = 5 * (step - 5)
        relay(KEYS, step)
        then = jnp.where(step == half - 1, done + 2, done + 3)
        lax.fori_loop(done, then, unit, 0)
        relay(VALUES, step)
        lax.fori_loop(then, jnp.minimum(done + 5, 2 * (half - 1)), unit, 0)
        return carry

    lax.fori_loop(5, half, steady, 0)
    gather_queries.drain()
    relay(KEYS, half)
    relay(VALUES, half)

    @pl.when(me >= half)
    def _():
        attend((me - half,), range(groups))

    for g in range(groups):
        mixed = (totals[g] / sums[g]).T
        for h in range(share):
            at = (g * share + h) * dim
            out[:, at : at + dim] = mixed[h * rows : (h + 1) * rows].astype(BF16)

    for kind in (KEYS, VALUES, GATES):
        for way in (UP, DOWN):
            hop(kind, way, last[kind, way], me).wait_send()


def on_device(tokens, query_weight, key_weight, value_weight, forget_weight, forget_bias):
    token_rows = tokens[0]
    rows, width = token_rows.shape
    ring = lax.axis_size("sp")
    heads = forget_weight.shape[1]
    dim = query_weight.shape[1] // heads
    groups = key_weight.shape[1] // dim
    share = heads // groups
    wide = -(-rows // 128) * 128
    vmem = pl.BlockSpec(memory_space=pltpu.VMEM)
    mixed = pl.pallas_call(
        kernel,
        out_shape=jax.ShapeDtypeStruct((rows, heads * dim), BF16),
        in_specs=[vmem] * 6,
        out_specs=vmem,
        scratch_shapes=[
            pltpu.VMEM((2, rows, width), BF16),
            pltpu.VMEM((width, heads * dim), BF16),
            pltpu.VMEM((width, groups * dim), BF16),
            pltpu.VMEM((width, groups * dim), BF16),
            pltpu.VMEM((ring, groups, rows, dim), BF16),
            pltpu.VMEM((ring, groups, rows, dim), BF16),
            pltpu.VMEM((ring, heads, wide), BF16),
            pltpu.VMEM((ring, rows, dim), BF16),
            pltpu.VMEM((groups, share * rows, 2 * dim), BF16),
            pltpu.VMEM((groups, dim, share * rows), F32),
            pltpu.VMEM((groups, 1, share * rows), F32),
            pltpu.VMEM((groups, 1, share * rows), F32),
            pltpu.SemaphoreType.DMA((3,)),
            pltpu.SemaphoreType.DMA((3, len(ITEM))),
            pltpu.SemaphoreType.DMA((3,)),
            pltpu.SemaphoreType.DMA((3,)),
            pltpu.SemaphoreType.DMA((3, 2, ring // 2)),
            pltpu.SemaphoreType.DMA((3, 2, ring // 2)),
            pltpu.SemaphoreType.DMA((2,)),
            pltpu.SemaphoreType.DMA((2,)),
        ],
        compiler_params=pltpu.CompilerParams(
            collective_id=0, has_side_effects=True, vmem_limit_bytes=32 * 2**20
        ),
    )(token_rows, query_weight, key_weight, value_weight, forget_weight.T, forget_bias[None, :])
    return mixed[None]


def solution(mesh):
    placed = (P("dp", "sp", None), P("dp", None), P("dp", None), P("dp", None), P(), P())
    return jax.shard_map(
        on_device, mesh=mesh, in_specs=placed, out_specs=P("dp", "sp", None), check_vma=False
    )
```

```python
import functools
import math

import jax
import jax.numpy as jnp
from jax import lax
from jax.experimental import pallas as pl
from jax.experimental.pallas import tpu as pltpu
from jax.sharding import PartitionSpec as P

BF16 = jnp.bfloat16
F32 = jnp.float32
MESH = pl.DeviceIdType.MESH
SIDE = 4
KEYS, VALUES, GATES = 0, 1, 2
UP, DOWN = 0, 1
NT = (((1,), (1,)), ((), ()))
TN = (((0,), (0,)), ((), ()))

WHOLE = [("W", 1, 0), ("W", 3, 0), ("W", 0, 1), ("W", 0, 3), ("W", 2, 0), ("W", 0, 2)]
HALVES = [(part, a, b) for part in "AB" for a in (1, 2, 3) for b in (1, 2, 3)]
OWN = ("W", 0, 0)
ITEM = {key: n for n, key in enumerate(WHOLE + HALVES)}


def copy_rows(part, depth):
    return depth if part == "W" else depth // 2


class Gather:
    def __init__(self, number, shard, full, sends, receives, pair_sends, pair_receives, place):
        self.number, self.shard, self.full = number, shard, full
        self.sems = (sends, receives, pair_sends, pair_receives)
        self.place = place
        self.depth = shard.shape[0]
        self.sent = 0

    def slot(self, a, b, other=False):
        x, y, core, turn = self.place
        if other:
            core, turn = 1 - core, -turn
        across = lax.rem(x + turn * a + 2 * SIDE, SIDE)
        along = lax.rem(y + turn * b + 2 * SIDE, SIDE)
        return (along * SIDE + across) * 2 + core

    def rows(self, key, other=False):
        part, a, b = key
        first = self.slot(a, b, other) * self.depth
        count = copy_rows(part, self.depth)
        if part == "B":
            first = first + count
        return self.full.at[pl.ds(pl.multiple_of(first, count), count)]

    def copy(self, key, received, target):
        sends, receives = self.sems[:2]
        n = ITEM[received]
        view = self.rows(key)
        return pltpu.make_async_remote_copy(
            src_ref=view,
            dst_ref=view,
            send_sem=sends.at[self.number],
            recv_sem=receives.at[self.number, n],
            device_id={"dp": target},
            device_id_type=MESH,
        )

    def send(self, key, dx, dy):
        part, a, b = key
        received = (part, (a - dx) % SIDE, (b - dy) % SIDE)
        copy = self.copy(key, received, self.slot(dx, dy))
        copy.start()
        self.sent += copy_rows(part, self.depth)

    def wait(self, key):
        self.copy(key, key, self.slot(1, 0)).wait_recv()

    def pair_copy(self, a, b, other=False):
        x, y, core, turn = self.place
        view = self.rows(("W", a, b), other)
        return pltpu.make_async_remote_copy(
            src_ref=view,
            dst_ref=view,
            send_sem=self.sems[2].at[self.number],
            recv_sem=self.sems[3].at[self.number],
            device_id={"dp": (y * SIDE + x) * 2 + 1 - core},
            device_id_type=MESH,
        )

    def share(self, a, b):
        self.pair_copy(a, b).start()

    def fetch(self, local_sem):
        self.fetched = pltpu.make_async_copy(self.shard, self.rows(OWN), local_sem)
        self.fetched.start()

    def begin(self):
        self.fetched.wait()
        for dx, dy in ((1, 0), (0, 1), (-1, 0), (0, -1)):
            self.send(OWN, dx, dy)
        self.share(0, 0)

    def first(self):
        for a in (3, 1):
            self.wait(("W", a, 0))
            if a == 3:
                self.send(("W", 3, 0), 1, 0)
            for dy in (1, -1):
                self.send(("A", a, 0), 0, dy)
            self.wait(("W", 0, a))
            if a == 3:
                self.send(("W", 0, 3), 0, 1)
            for dx in (1, -1):
                self.send(("B", 0, a), dx, 0)
            self.share(a, 0)
            self.share(0, a)

    def second(self):
        for a in (3, 1):
            self.wait(("A", a, 3))
            self.send(("A", a, 3), 0, 1)
            self.wait(("B", 3, a))
            self.send(("B", 3, a), 1, 0)
        self.wait(("W", 2, 0))
        for dy in (1, -1):
            self.send(("A", 2, 0), 0, dy)
        self.wait(("W", 0, 2))
        for dx in (1, -1):
            self.send(("B", 0, 2), dx, 0)
        self.share(2, 0)
        self.share(0, 2)
        for a in (3, 1):
            self.wait(("A", a, 1))
            self.wait(("B", 1, a))
        for a in (3, 1):
            for b in (3, 1):
                self.share(a, b)

    def third(self):
        self.wait(("A", 2, 3))
        self.send(("A", 2, 3), 0, 1)
        self.wait(("B", 3, 2))
        self.send(("B", 3, 2), 1, 0)
        for a in (3, 1):
            self.wait(("A", a, 2))
            self.wait(("B", 2, a))
        self.wait(("A", 2, 1))
        self.wait(("B", 1, 2))
        for a in (3, 1):
            self.share(2, a)
            self.share(a, 2)

    def fourth(self):
        self.wait(("A", 2, 2))
        self.wait(("B", 2, 2))
        self.share(2, 2)

    def bulk(self, rows, send_sem, receive_sem):
        view = self.full.at[pl.ds(0, rows)]
        return pltpu.make_async_remote_copy(
            src_ref=view,
            dst_ref=view,
            send_sem=send_sem.at[self.number],
            recv_sem=receive_sem.at[self.number],
            device_id={"dp": self.slot(1, 0)},
            device_id_type=MESH,
        )

    def complete(self):
        self.bulk(SIDE * SIDE * self.depth, self.sems[2], self.sems[3]).wait_recv()

    def drain(self):
        self.bulk(self.sent, self.sems[0], self.sems[3]).wait_send()
        self.bulk(SIDE * SIDE * self.depth, self.sems[2], self.sems[3]).wait_send()


def kernel(
    tokens_in, query_shard, key_shard, value_shard, forget_in, bias_in, out,
    tokens, forget_weight, forget_bias, near, between, chances, query_all, key_all, value_all, keys, values, gates, key_extra, queries, totals, peaks, sums,
    sends, receives, pair_sends, pair_receives, ring_sends, ring_receives, near_sends, near_receives, local_sems,
):
    ring = lax.axis_size("sp")
    half = ring // 2
    me = lax.axis_index("sp")
    mine = lax.axis_index("dp")
    core = lax.rem(mine, 2)
    x = lax.rem(lax.div(mine, 2), SIDE)
    y = lax.div(mine, 2 * SIDE)
    place = (x, y, core, 1 - 2 * core)
    rows = tokens.shape[0]
    heads = forget_weight.shape[0]
    groups, dim = keys.shape[1], keys.shape[3]
    share = heads // groups
    root = math.sqrt(dim)

    part_width = query_all.shape[2]
    gather_keys, gather_values, gather_left, gather_right = (
        Gather(n, shard, full, sends, receives, pair_sends, pair_receives, place)
        for n, (shard, full) in enumerate(
            (
                (key_shard, key_all),
                (value_shard, value_all),
                (query_shard.at[:, pl.ds(0, part_width)], query_all.at[0]),
                (query_shard.at[:, pl.ds(part_width, part_width)], query_all.at[1]),
            )
        )
    )

    above, below = lax.rem(me + 1, ring), lax.rem(me + ring - 1, ring)
    barrier = pltpu.get_barrier_semaphore()
    for dx, dy in ((1, 0), (0, 1), (-1, 0), (0, -1)):
        pl.semaphore_signal(
            barrier, inc=1, device_id={"dp": gather_keys.slot(dx, dy)}, device_id_type=MESH
        )
    pl.semaphore_signal(barrier, inc=1, device_id={"dp": mine + 1 - 2 * core}, device_id_type=MESH)
    for neighbour in (above, below):
        pl.semaphore_signal(barrier, inc=1, device_id={"sp": neighbour}, device_id_type=MESH)
    gather_keys.fetch(local_sems.at[0])
    fetches = [
        pltpu.make_async_copy(source, target, local_sems.at[n + 3])
        for n, (source, target) in enumerate(
            ((tokens_in, tokens), (forget_in, forget_weight), (bias_in, forget_bias))
        )
    ]
    for fetch in fetches:
        fetch.start()
    gather_values.fetch(local_sems.at[1])
    gather_left.fetch(local_sems.at[2])
    gather_right.fetch(local_sems.at[6])
    pl.semaphore_wait(barrier, 7)

    buffers = {KEYS: keys, VALUES: values, GATES: gates}
    last = {
        (KEYS, UP): half, (KEYS, DOWN): half,
        (VALUES, UP): half, (VALUES, DOWN): half,
        (GATES, UP): half, (GATES, DOWN): half - 1,
    }

    def hop(kind, way, step, slot):
        view = buffers[kind].at[slot]
        if kind != GATES and isinstance(step, int) and step == half:
            view = buffers[kind].at[slot, pl.ds(0, groups - 1) if way == UP else pl.ds(groups - 1, 1)]
        return pltpu.make_async_remote_copy(
            src_ref=view,
            dst_ref=view,
            send_sem=ring_sends.at[kind, way, step - 1],
            recv_sem=ring_receives.at[kind, way, step - 1],
            device_id={"sp": above if way == UP else below},
            device_id_type=MESH,
        )

    def origin(way, step):
        return lax.rem(me - step + ring, ring) if way == UP else lax.rem(me + step, ring)

    def fresh(kind, way, step):
        if way == UP:
            return me >= step
        return (me + step >= ring) | (me + step < last[kind, way])

    def passed(kind, way, step):
        return (me >= step) & (me < ring - 1) if way == UP else fresh(kind, way, step)

    def launch(kind, way):
        @pl.when(passed(kind, way, 1))
        def _():
            hop(kind, way, 2, origin(way, 1)).start()

    def first_hop(way, part, slot):
        view = keys.at[slot, :, pl.ds(part * (rows // 2), rows // 2)]
        return pltpu.make_async_remote_copy(
            src_ref=view,
            dst_ref=view,
            send_sem=ring_sends.at[KEYS, way, part],
            recv_sem=ring_receives.at[KEYS, way, part],
            device_id={"sp": above if way == UP else below},
            device_id_type=MESH,
        )

    def launch_keys(way, part):
        @pl.when(passed(KEYS, way, 1))
        def _():
            first_hop(way, part, origin(way, 1)).start()

    def relay(kind, step):
        for way in (UP, DOWN):
            final = last[kind, way]
            slot = origin(way, step)
            fixed = isinstance(step, int)
            if fixed and step > final:
                continue

            @pl.when(fresh(kind, way, step))
            def _():
                if fixed and kind == KEYS and step == 2:
                    first_hop(way, 0, slot).wait_recv()
                    first_hop(way, 1, slot).wait_recv()
                else:
                    hop(kind, way, step, slot).wait_recv()

            if not fixed or step < final:

                @pl.when(passed(kind, way, step))
                def _():
                    if fixed:
                        hop(kind, way, step + 1, slot).start()
                    else:

                        @pl.when(step < half - 1)
                        def _():
                            hop(kind, way, step + 1, slot).start()

                        @pl.when(step == half - 1)
                        def _():
                            hop(kind, way, half, slot).start()

            if not fixed or step >= 3:

                @pl.when(passed(kind, way, step - 2))
                def _():
                    if fixed and kind == KEYS and step == 3:
                        first_hop(way, 0, slot).wait_send()
                        first_hop(way, 1, slot).wait_send()
                    else:
                        hop(kind, way, step - 1, slot).wait_send()

    def visit(way, part):
        these = pl.ds(part * (rows // 2), rows // 2)
        return pltpu.make_async_remote_copy(
            src_ref=tokens.at[these],
            dst_ref=near.at[way, these],
            send_sem=near_sends.at[way, part],
            recv_sem=near_receives.at[way, part],
            device_id={"sp": above if way == UP else below},
            device_id_type=MESH,
        )

    def visits(act):
        for part in (0, 1):
            for way, goes in ((UP, me < ring - 1), (DOWN, me < half)):

                @pl.when(goes)
                def _():
                    act(visit(way, part))

    comes = {UP: me >= 1, DOWN: (me == ring - 1) | (me < half - 1)}

    def meet(way, part):
        @pl.when(comes[way])
        def _():
            visit(way, part).wait_recv()
            project(near.at[way], key_all, keys, origin(way, 1), part * (rows // 2), rows // 2)

    def meet_gates(way):
        @pl.when(comes[way])
        def _():
            gate(near.at[way], origin(way, 1))

    def meet_values(way):
        @pl.when(comes[way])
        def _():
            project(near.at[way], value_all, values, origin(way, 1))

    wide = gates.shape[2]
    eye = (
        lax.broadcasted_iota(jnp.int32, (rows, wide), 0) == lax.broadcasted_iota(jnp.int32, (rows, wide), 1)
    ).astype(F32).astype(BF16)

    def gate(source, block):
        bias_at = lax.broadcasted_iota(jnp.int32, (heads, heads), 0) == lax.broadcasted_iota(jnp.int32, (heads, heads), 1)
        bias = jnp.sum(jnp.where(bias_at, forget_bias[...], 0.0), axis=1, keepdims=True)
        gate_input = lax.dot_general(forget_weight[...], source[...], NT, preferred_element_type=F32) + bias
        log_gate = (jnp.minimum(gate_input, 0.0) - jnp.log1p(jnp.exp(-jnp.abs(gate_input)))).astype(BF16)
        gates[block] = jnp.dot(log_gate, eye, preferred_element_type=F32).astype(BF16)

    def project(source, weight, buffer, block, first=0, count=rows):
        def one(g, carry):
            columns = pl.ds(pl.multiple_of(g * dim * 2, dim * 2), dim * 2)
            these = source[pl.ds(first, count), :]
            part = jnp.dot(these, weight[:, columns], preferred_element_type=F32).astype(BF16)
            buffer[block, 2 * g, pl.ds(first, count)] = part[:, :dim]
            buffer[block, 2 * g + 1, pl.ds(first, count)] = part[:, dim:]
            return carry

        lax.fori_loop(0, groups // 2, one, 0)

    lane = lax.broadcasted_iota(jnp.int32, (rows, dim), 1)
    tall = rows + 8
    down = lax.broadcasted_iota(jnp.int32, (tall, wide), 0)
    right = lax.broadcasted_iota(jnp.int32, (tall, wide), 1)
    later = ((right > down) | (down >= rows)).astype(F32).astype(BF16)
    sofar = ((right <= down) & (down < rows)).astype(F32).astype(BF16)

    def thrice(block):
        g = gates[block]
        return jnp.concatenate([g, g, g, jnp.zeros((dim - 3 * heads, wide), BF16)], axis=0)

    def parts(exact):
        hi = exact.astype(BF16).astype(F32)
        rest = exact - hi
        mid = rest.astype(BF16).astype(F32)
        low = rest - mid
        return jnp.where(
            lane < heads, hi, jnp.where(lane < 2 * heads, mid, jnp.where(lane < 3 * heads, low, 0.0))
        )

    ones = ((lane >= 3 * heads) & (lane < 3 * heads + 3)).astype(F32)

    def decay_of(step, carry):
        @pl.when(me >= step)
        def _():
            block = lax.rem(me - step + ring, ring)
            summed = lax.dot_general(later, thrice(block), NT, preferred_element_type=F32)
            after = between[...]
            key_extra[block] = (parts((summed[:rows] + after) * root) + ones).astype(BF16)
            between[...] = after + summed[rows : rows + 1]

        return carry

    def decay_own():
        between[...] = -lax.dot_general(later, thrice(me), NT, preferred_element_type=F32)[rows : rows + 1]
        decay_of(0, 0)

    def query_extras(first, end):
        own_sum = lax.dot_general(sofar, thrice(me), NT, preferred_element_type=F32)[:rows]
        own_parts = parts(own_sum * root).astype(BF16)
        pick_row = lax.broadcasted_iota(jnp.int32, (dim, dim), 0)
        pick_lane = lax.broadcasted_iota(jnp.int32, (dim, dim), 1)

        def query_extra(h, carry):
            pick = ((pick_row == h + heads * (pick_lane - 3 * heads)) & (pick_lane >= 3 * heads)
                    & (pick_lane < 3 * heads + 3)).astype(F32).astype(BF16)
            moved = jnp.dot(own_parts, pick, preferred_element_type=F32)
            hot = ((lane == h) | (lane == h + heads) | (lane == h + 2 * heads)).astype(F32)
            place_rows = pl.ds(pl.multiple_of(lax.rem(h, share) * rows, rows), rows)
            queries[lax.div(h, share), place_rows, dim:] = (moved + hot).astype(BF16)
            return carry

        lax.fori_loop(first, end, query_extra, 0)

    def query_group(g, carry):
        at = pl.multiple_of(lax.rem(g, groups // 2) * dim * share, dim * share)
        weight = query_all[lax.div(g, groups // 2), :, pl.ds(at, dim * share)]
        part = jnp.dot(tokens[...], weight, preferred_element_type=F32).astype(BF16)
        for h in range(share):
            queries[g, h * rows : (h + 1) * rows, :dim] = part[:, h * dim : (h + 1) * dim]
        return carry

    scale = math.log2(math.e) / root
    breadth = share * rows

    def attend(blocks, some_groups, diagonal=False):
        key_rows = rows * len(blocks)
        for g in some_groups:
            key_part = jnp.concatenate(
                [jnp.concatenate([keys[block, g], key_extra[block]], axis=1) for block in blocks], axis=0
            )
            value_part = jnp.concatenate([values[block, g] for block in blocks], axis=0)
            score = lax.dot_general(key_part, queries[g], NT, preferred_element_type=F32)
            if diagonal:
                key_at = lax.broadcasted_iota(jnp.int32, (key_rows, breadth), 0)
                query_at = lax.broadcasted_iota(jnp.int32, (key_rows, breadth), 1)
                for h in range(share - 1, 0, -1):
                    query_at = jnp.where(query_at >= h * rows, query_at - h * rows, query_at)
                score = jnp.where(key_at <= query_at, score, -jnp.inf)
                peak = jnp.max(score, axis=0, keepdims=True)
            else:
                old = peaks[g]
                peak = jnp.maximum(old, jnp.max(score, axis=0, keepdims=True))
            weight = jnp.exp2((score - peak) * scale)
            total = jnp.sum(weight, axis=0, keepdims=True)
            mixed = lax.dot_general(value_part, weight.astype(BF16), TN, preferred_element_type=F32)
            peaks[g] = peak
            if diagonal:
                sums[g] = total
                totals[g] = mixed
            else:
                fade = jnp.exp2((old - peak) * scale)
                sums[g] = sums[g] * fade + total
                totals[g] = totals[g] * fade + mixed

    def attend_own(n, carry):
        attend((me,), (2 * n, 2 * n + 1), diagonal=True)
        return carry

    def unit(u, carry):
        pair = lax.div(u, 2)
        some = (2 * lax.rem(u, 2), 2 * lax.rem(u, 2) + 1)
        over = (pair == 2) | (pair == 3) | (pair == 5)
        step = jnp.where(pair < 2, 2 * pair + 1, jnp.where(pair < 4, 2 * pair - 3, jnp.where(pair < 6, 5, 7)))
        one = jnp.where(over, me + step - ring, me - step)
        two = jnp.where(pair == 6, me + step - ring, jnp.where(over, me + step + 1 - ring, me - step - 1))

        @pl.when((one >= 0) & (two >= 0))
        def _():
            attend((one, two), some)

        @pl.when(((one >= 0) | (two >= 0)) & ((one < 0) | (two < 0)))
        def _():
            attend((jnp.maximum(one, two),), some)

        return carry

    gather_keys.begin()
    for fetch in fetches:
        fetch.wait()
    visits(lambda copy: copy.start())
    gate(tokens, me)
    gather_keys.first()
    gather_values.begin()
    decay_own()
    gather_keys.second()
    gather_values.first()
    gather_keys.third()
    gather_values.second()
    gather_keys.fourth()
    gather_keys.complete()
    meet(DOWN, 0)
    meet(UP, 0)
    project(tokens, key_all, keys, me, 0, rows // 2)
    launch_keys(DOWN, 0)
    launch_keys(UP, 0)
    gather_values.third()
    gather_left.begin()
    gather_right.begin()
    meet(UP, 1)
    meet_gates(UP)
    launch(GATES, UP)
    meet(DOWN, 1)
    launch_keys(UP, 1)
    meet_gates(DOWN)
    launch_keys(DOWN, 1)
    gather_values.fourth()
    launch(GATES, DOWN)
    gather_values.complete()
    meet_values(UP)
    meet_values(DOWN)
    launch(VALUES, UP)
    project(tokens, key_all, keys, me, rows // 2, rows // 2)
    launch(VALUES, DOWN)
    gather_left.first()
    relay(GATES, 2)
    relay(KEYS, 2)
    gather_right.first()
    project(tokens, value_all, values, me)
    query_extras(0, heads)
    relay(GATES, 3)
    relay(VALUES, 2)
    gather_left.second()
    relay(GATES, 4)
    relay(KEYS, 3)
    gather_keys.drain()
    gather_values.drain()
    lax.fori_loop(1, 4, decay_of, 0)
    gather_right.second()
    lax.fori_loop(4, 5, decay_of, 0)
    relay(GATES, 5)
    relay(VALUES, 3)
    gather_left.third()
    visits(lambda copy: copy.wait_send())
    lax.fori_loop(5, 6, decay_of, 0)
    relay(GATES, 6)
    relay(KEYS, 4)
    gather_left.fourth()
    gather_right.third()
    lax.fori_loop(6, 7, decay_of, 0)
    gather_right.fourth()
    relay(GATES, 7)
    relay(VALUES, 4)
    gather_left.complete()
    gather_right.complete()
    lax.fori_loop(0, groups, query_group, 0)
    lax.fori_loop(0, groups // 2, attend_own, 0)
    relay(GATES, 8)
    relay(KEYS, 5)
    lax.fori_loop(7, ring, decay_of, 0)
    lax.fori_loop(0, 2, unit, 0)
    relay(VALUES, 5)
    lax.fori_loop(2, 4, unit, 0)

    def steady(step, carry):
        done = 5 * (step - 6) + 4
        relay(KEYS, step)
        lax.fori_loop(done, done + 3, unit, 0)
        relay(VALUES, step)
        lax.fori_loop(done + 3, done + 5, unit, 0)
        return carry

    lax.fori_loop(6, half, steady, 0)
    gather_left.drain()
    gather_right.drain()
    relay(KEYS, half)

    @pl.when(me >= half)
    def _():
        block = me - half
        for g in range(groups):
            key_part = jnp.concatenate([keys[block, g], key_extra[block]], axis=1)
            score = lax.dot_general(key_part, queries[g], NT, preferred_element_type=F32)
            old = peaks[g]
            peak = jnp.maximum(old, jnp.max(score, axis=0, keepdims=True))
            weight = jnp.exp2((score - peak) * scale)
            fade = jnp.exp2((old - peak) * scale)
            sums[g] = sums[g] * fade + jnp.sum(weight, axis=0, keepdims=True)
            totals[g] = totals[g] * fade
            chances[g] = weight.astype(BF16)

    relay(VALUES, half)

    @pl.when(me >= half)
    def _():
        for g in range(groups):
            totals[g] += lax.dot_general(values[me - half, g], chances[g], TN, preferred_element_type=F32)

    for g in range(groups):
        mixed = (totals[g] / sums[g]).T
        for h in range(share):
            at = (g * share + h) * dim
            out[:, at : at + dim] = mixed[h * rows : (h + 1) * rows].astype(BF16)

    for kind in (KEYS, VALUES, GATES):
        for way in (UP, DOWN):

            @pl.when(passed(kind, way, last[kind, way] - 1))
            def _():
                hop(kind, way, last[kind, way], me).wait_send()


def on_device(tokens, query_weight, key_weight, value_weight, forget_weight, forget_bias):
    token_rows = tokens[0]
    rows, width = token_rows.shape
    ring = lax.axis_size("sp")
    heads = forget_weight.shape[1]
    dim = query_weight.shape[1] // heads
    groups = key_weight.shape[1] // dim
    share = heads // groups
    wide = -(-rows // 128) * 128
    vmem = pl.BlockSpec(memory_space=pltpu.VMEM)
    inputs = (token_rows, query_weight, key_weight, value_weight, forget_weight.T, forget_bias[None, :])
    inputs = tuple(pltpu.with_memory_space_constraint(a, pltpu.HBM) for a in inputs)
    mixed = pl.pallas_call(
        kernel,
        out_shape=jax.ShapeDtypeStruct((rows, heads * dim), BF16),
        in_specs=[pl.BlockSpec(memory_space=pltpu.HBM)] * 6,
        out_specs=vmem,
        scratch_shapes=[
            pltpu.VMEM((rows, width), BF16),
            pltpu.VMEM((heads, width), BF16),
            pltpu.VMEM((1, heads), F32),
            pltpu.VMEM((2, rows, width), BF16),
            pltpu.VMEM((1, dim), F32),
            pltpu.VMEM((groups, rows, share * rows), BF16),
            pltpu.VMEM((2, width, heads * dim // 2), BF16),
            pltpu.VMEM((width, groups * dim), BF16),
            pltpu.VMEM((width, groups * dim), BF16),
            pltpu.VMEM((ring, groups, rows, dim), BF16),
            pltpu.VMEM((ring, groups, rows, dim), BF16),
            pltpu.VMEM((ring, heads, wide), BF16),
            pltpu.VMEM((ring, rows, dim), BF16),
            pltpu.VMEM((groups, share * rows, 2 * dim), BF16),
            pltpu.VMEM((groups, dim, share * rows), F32),
            pltpu.VMEM((groups, 1, share * rows), F32),
            pltpu.VMEM((groups, 1, share * rows), F32),
            pltpu.SemaphoreType.DMA((4,)),
            pltpu.SemaphoreType.DMA((4, len(ITEM))),
            pltpu.SemaphoreType.DMA((4,)),
            pltpu.SemaphoreType.DMA((4,)),
            pltpu.SemaphoreType.DMA((3, 2, ring // 2)),
            pltpu.SemaphoreType.DMA((3, 2, ring // 2)),
            pltpu.SemaphoreType.DMA((2, 2)),
            pltpu.SemaphoreType.DMA((2, 2)),
            pltpu.SemaphoreType.DMA((7,)),
        ],
        compiler_params=pltpu.CompilerParams(
            collective_id=0, has_side_effects=True, vmem_limit_bytes=32 * 2**20
        ),
    )(*inputs)
    return mixed[None]


def solution(mesh):
    placed = (P("dp", "sp", None), P("dp", None), P("dp", None), P("dp", None), P(), P())
    return jax.shard_map(
        on_device, mesh=mesh, in_specs=placed, out_specs=P("dp", "sp", None), check_vma=False
    )
```

```python
import functools
import math

import jax
import jax.numpy as jnp
from jax import lax
from jax.experimental import pallas as pl
from jax.experimental.pallas import tpu as pltpu
from jax.sharding import PartitionSpec as P

BF16 = jnp.bfloat16
F32 = jnp.float32
MESH = pl.DeviceIdType.MESH
SIDE = 4
KEYS, VALUES, GATES = 0, 1, 2
UP, DOWN = 0, 1
NT = (((1,), (1,)), ((), ()))
TN = (((0,), (0,)), ((), ()))

GROUPS = [
    [("W", 3, 0), ("W", 0, 3)],
    [("W", 1, 0), ("W", 0, 1)],
    [("A", 3, 3), ("A", 1, 3), ("B", 3, 3), ("B", 3, 1)],
    [("W", 2, 0), ("W", 0, 2)],
    [("A", 3, 1), ("A", 1, 1), ("B", 1, 3), ("B", 1, 1)],
    [("A", 2, 3), ("B", 3, 2)],
    [("A", 3, 2), ("A", 1, 2), ("B", 2, 3), ("B", 2, 1), ("A", 2, 1), ("B", 1, 2)],
    [("A", 2, 2), ("B", 2, 2)],
]
OWN = ("W", 0, 0)
ITEM = {key: n for n, group in enumerate(GROUPS) for key in group}


def copy_rows(part, depth):
    return depth if part == "W" else depth // 2


class Gather:
    def __init__(self, number, shard, full, sends, receives, pair_sends, pair_receives, place):
        self.number, self.shard, self.full = number, shard, full
        self.sems = (sends, receives, pair_sends, pair_receives)
        self.place = place
        self.depth = shard.shape[0]
        self.sent = 0

    def slot(self, a, b, other=False):
        x, y, core, turn = self.place
        if other:
            core, turn = 1 - core, -turn
        across = lax.rem(x + turn * a + 2 * SIDE, SIDE)
        along = lax.rem(y + turn * b + 2 * SIDE, SIDE)
        return (along * SIDE + across) * 2 + core

    def rows(self, key, other=False):
        part, a, b = key
        first = self.slot(a, b, other) * self.depth
        count = copy_rows(part, self.depth)
        if part == "B":
            first = first + count
        return self.full.at[pl.ds(pl.multiple_of(first, count), count)]

    def copy(self, key, received, target):
        sends, receives = self.sems[:2]
        n = ITEM[received]
        view = self.rows(key)
        return pltpu.make_async_remote_copy(
            src_ref=view,
            dst_ref=view,
            send_sem=sends.at[self.number],
            recv_sem=receives.at[self.number, n],
            device_id={"dp": target},
            device_id_type=MESH,
        )

    def send(self, key, dx, dy):
        part, a, b = key
        received = (part, (a - dx) % SIDE, (b - dy) % SIDE)
        copy = self.copy(key, received, self.slot(dx, dy))
        copy.start()
        self.sent += copy_rows(part, self.depth)

    def wait(self, group):
        rows = sum(copy_rows(key[0], self.depth) for key in GROUPS[group])
        self.bulk(rows, self.sems[0].at[self.number], self.sems[1].at[self.number, group]).wait_recv()

    def pair_copy(self, a, b, other=False):
        x, y, core, turn = self.place
        view = self.rows(("W", a, b), other)
        return pltpu.make_async_remote_copy(
            src_ref=view,
            dst_ref=view,
            send_sem=self.sems[2].at[self.number],
            recv_sem=self.sems[3].at[self.number],
            device_id={"dp": (y * SIDE + x) * 2 + 1 - core},
            device_id_type=MESH,
        )

    def share(self, a, b):
        self.pair_copy(a, b).start()

    def fetch(self, local_sem):
        self.fetched = pltpu.make_async_copy(self.shard, self.rows(OWN), local_sem)
        self.fetched.start()

    def begin(self):
        self.fetched.wait()
        for dx, dy in ((1, 0), (0, 1), (-1, 0), (0, -1)):
            self.send(OWN, dx, dy)
        self.share(0, 0)

    def first(self):
        self.wait(0)
        self.send(("W", 3, 0), 1, 0)
        self.send(("W", 0, 3), 0, 1)
        for a in (3, 1):
            if a == 1:
                self.wait(1)
            for way in (1, -1):
                self.send(("A", a, 0), 0, way)
                self.send(("B", 0, a), way, 0)
            self.share(a, 0)
            self.share(0, a)

    def second(self):
        self.wait(2)
        for a in (3, 1):
            self.send(("A", a, 3), 0, 1)
            self.send(("B", 3, a), 1, 0)
        self.wait(3)
        for way in (1, -1):
            self.send(("A", 2, 0), 0, way)
            self.send(("B", 0, 2), way, 0)
        self.share(2, 0)
        self.share(0, 2)
        self.wait(4)
        for a in (3, 1):
            for b in (3, 1):
                self.share(a, b)

    def third(self):
        self.wait(5)
        self.send(("A", 2, 3), 0, 1)
        self.send(("B", 3, 2), 1, 0)
        self.wait(6)
        for a in (3, 1):
            self.share(2, a)
            self.share(a, 2)

    def fourth(self):
        self.wait(7)
        self.share(2, 2)

    def bulk(self, rows, send_sem, receive_sem):
        view = self.full.at[pl.ds(0, rows)]
        return pltpu.make_async_remote_copy(
            src_ref=view,
            dst_ref=view,
            send_sem=send_sem,
            recv_sem=receive_sem,
            device_id={"dp": self.slot(1, 0)},
            device_id_type=MESH,
        )

    def complete(self):
        n = self.number
        self.bulk(SIDE * SIDE * self.depth, self.sems[2].at[n], self.sems[3].at[n]).wait_recv()

    def drain(self):
        n = self.number
        self.bulk(self.sent, self.sems[0].at[n], self.sems[3].at[n]).wait_send()
        self.bulk(SIDE * SIDE * self.depth, self.sems[2].at[n], self.sems[3].at[n]).wait_send()


def kernel(
    tokens_in, query_shard, key_shard, value_shard, forget_in, bias_in, out,
    tokens, forget_weight, forget_bias, near, between, chances, query_all, key_all, value_all, keys, values, gates, key_extra, queries, totals, peaks, sums,
    sends, receives, pair_sends, pair_receives, ring_sends, ring_receives, near_sends, near_receives, local_sems,
):
    ring = lax.axis_size("sp")
    half = ring // 2
    me = lax.axis_index("sp")
    mine = lax.axis_index("dp")
    core = lax.rem(mine, 2)
    x = lax.rem(lax.div(mine, 2), SIDE)
    y = lax.div(mine, 2 * SIDE)
    place = (x, y, core, 1 - 2 * core)
    rows = tokens.shape[0]
    heads = forget_weight.shape[0]
    groups, dim = keys.shape[1], keys.shape[3]
    share = heads // groups
    root = math.sqrt(dim)

    part_width = query_all.shape[2]
    gather_keys, gather_values, gather_left, gather_right = (
        Gather(n, shard, full, sends, receives, pair_sends, pair_receives, place)
        for n, (shard, full) in enumerate(
            (
                (key_shard, key_all),
                (value_shard, value_all),
                (query_shard.at[:, pl.ds(0, part_width)], query_all.at[0]),
                (query_shard.at[:, pl.ds(part_width, part_width)], query_all.at[1]),
            )
        )
    )

    above, below = lax.rem(me + 1, ring), lax.rem(me + ring - 1, ring)
    barrier = pltpu.get_barrier_semaphore()
    for dx, dy in ((1, 0), (0, 1), (-1, 0), (0, -1)):
        pl.semaphore_signal(
            barrier, inc=1, device_id={"dp": gather_keys.slot(dx, dy)}, device_id_type=MESH
        )
    pl.semaphore_signal(barrier, inc=1, device_id={"dp": mine + 1 - 2 * core}, device_id_type=MESH)
    for neighbour in (above, below):
        pl.semaphore_signal(barrier, inc=1, device_id={"sp": neighbour}, device_id_type=MESH)
    gather_keys.fetch(local_sems.at[0])
    fetches = [
        pltpu.make_async_copy(source, target, local_sems.at[n + 3])
        for n, (source, target) in enumerate(
            ((tokens_in, tokens), (forget_in, forget_weight), (bias_in, forget_bias))
        )
    ]
    for fetch in fetches:
        fetch.start()
    gather_values.fetch(local_sems.at[1])
    gather_left.fetch(local_sems.at[2])
    gather_right.fetch(local_sems.at[6])
    pl.semaphore_wait(barrier, 7)

    buffers = {KEYS: keys, VALUES: values, GATES: gates}
    last = {
        (KEYS, UP): half, (KEYS, DOWN): half,
        (VALUES, UP): half, (VALUES, DOWN): half,
        (GATES, UP): half, (GATES, DOWN): half - 1,
    }

    def hop(kind, way, step, slot):
        view = buffers[kind].at[slot]
        if kind != GATES and isinstance(step, int) and step == half:
            view = buffers[kind].at[slot, pl.ds(0, groups - 1) if way == UP else pl.ds(groups - 1, 1)]
        return pltpu.make_async_remote_copy(
            src_ref=view,
            dst_ref=view,
            send_sem=ring_sends.at[kind, way, step % 2 if isinstance(step, int) else lax.rem(step, 2)],
            recv_sem=ring_receives.at[kind, way, step - 1],
            device_id={"sp": above if way == UP else below},
            device_id_type=MESH,
        )

    def origin(way, step):
        return lax.rem(me - step + ring, ring) if way == UP else lax.rem(me + step, ring)

    def fresh(kind, way, step):
        if way == UP:
            return me >= step
        return (me + step >= ring) | (me + step < last[kind, way])

    def passed(kind, way, step):
        return (me >= step) & (me < ring - 1) if way == UP else fresh(kind, way, step)

    def launch(kind, way):
        @pl.when(passed(kind, way, 1))
        def _():
            hop(kind, way, 2, origin(way, 1)).start()

    def first_hop(kind, way, part, slot):
        view = (
            keys.at[slot, :, pl.ds(part * (rows // 2), rows // 2)]
            if kind == KEYS
            else values.at[slot, pl.ds(part * (groups // 2), groups // 2)]
        )
        return pltpu.make_async_remote_copy(
            src_ref=view,
            dst_ref=view,
            send_sem=ring_sends.at[kind, way, part],
            recv_sem=ring_receives.at[kind, way, part],
            device_id={"sp": above if way == UP else below},
            device_id_type=MESH,
        )

    def launch_part(kind, way, part):
        @pl.when(passed(kind, way, 1))
        def _():
            first_hop(kind, way, part, origin(way, 1)).start()

    def relay(kind, step):
        for way in (UP, DOWN):
            final = last[kind, way]
            slot = origin(way, step)
            fixed = isinstance(step, int)
            if fixed and step > final:
                continue
            begins = fixed and step == 2 and kind != GATES

            @pl.when(fresh(kind, way, step))
            def _():
                if begins:
                    first_hop(kind, way, 0, slot).wait_recv()
                    first_hop(kind, way, 1, slot).wait_recv()
                else:
                    hop(kind, way, step, slot).wait_recv()

            if begins:

                @pl.when(passed(kind, way, 1))
                def _():
                    first_hop(kind, way, 0, slot).wait_send()
                    first_hop(kind, way, 1, slot).wait_send()

            elif not fixed or step > 3 or (step == 3 and kind == GATES):

                @pl.when(passed(kind, way, step - 2))
                def _():
                    hop(kind, way, step - 1, slot).wait_send()

            if not fixed or step < final:

                @pl.when(passed(kind, way, step))
                def _():
                    if fixed:
                        hop(kind, way, step + 1, slot).start()
                    else:

                        @pl.when(step < half - 1)
                        def _():
                            hop(kind, way, step + 1, slot).start()

                        @pl.when(step == half - 1)
                        def _():
                            hop(kind, way, half, slot).start()

    def visit(way, part):
        these = pl.ds(part * (rows // 2), rows // 2)
        return pltpu.make_async_remote_copy(
            src_ref=tokens.at[these],
            dst_ref=near.at[way, these],
            send_sem=near_sends.at[way, part],
            recv_sem=near_receives.at[way, part],
            device_id={"sp": above if way == UP else below},
            device_id_type=MESH,
        )

    def visits(act):
        for part in (0, 1):
            for way, goes in ((UP, me < ring - 1), (DOWN, me < half)):

                @pl.when(goes)
                def _():
                    act(visit(way, part))

    comes = {UP: me >= 1, DOWN: (me == ring - 1) | (me < half - 1)}

    def meet(way, part):
        @pl.when(comes[way])
        def _():
            visit(way, part).wait_recv()
            project(near.at[way], key_all, keys, origin(way, 1), part * (rows // 2), rows // 2)

    def meet_gates(way):
        @pl.when(comes[way])
        def _():
            gate(near.at[way], origin(way, 1))

    def meet_values(way, part):
        @pl.when(comes[way])
        def _():
            project(near.at[way], value_all, values, origin(way, 1), some=(part, part + 1))

    wide = gates.shape[2]
    eye = (
        lax.broadcasted_iota(jnp.int32, (rows, wide), 0) == lax.broadcasted_iota(jnp.int32, (rows, wide), 1)
    ).astype(F32).astype(BF16)

    def gate(source, block):
        bias_at = lax.broadcasted_iota(jnp.int32, (heads, heads), 0) == lax.broadcasted_iota(jnp.int32, (heads, heads), 1)
        bias = jnp.sum(jnp.where(bias_at, forget_bias[...], 0.0), axis=1, keepdims=True)
        gate_input = lax.dot_general(forget_weight[...], source[...], NT, preferred_element_type=F32) + bias
        log_gate = (jnp.minimum(gate_input, 0.0) - jnp.log1p(jnp.exp(-jnp.abs(gate_input)))).astype(BF16)
        gates[block] = jnp.dot(log_gate, eye, preferred_element_type=F32).astype(BF16)

    def project(source, weight, buffer, block, first=0, count=rows, some=(0, groups // 2)):
        def one(g, carry):
            columns = pl.ds(pl.multiple_of(g * dim * 2, dim * 2), dim * 2)
            these = source[pl.ds(first, count), :]
            part = jnp.dot(these, weight[:, columns], preferred_element_type=F32).astype(BF16)
            buffer[block, 2 * g, pl.ds(first, count)] = part[:, :dim]
            buffer[block, 2 * g + 1, pl.ds(first, count)] = part[:, dim:]
            return carry

        lax.fori_loop(some[0], some[1], one, 0)

    lane = lax.broadcasted_iota(jnp.int32, (rows, dim), 1)
    tall = rows + 8
    down = lax.broadcasted_iota(jnp.int32, (tall, wide), 0)
    right = lax.broadcasted_iota(jnp.int32, (tall, wide), 1)
    later = ((right > down) | (down >= rows)).astype(F32).astype(BF16)
    sofar = ((right <= down) & (down < rows)).astype(F32).astype(BF16)

    def thrice(block):
        g = gates[block]
        return jnp.concatenate([g, g, g, jnp.zeros((dim - 3 * heads, wide), BF16)], axis=0)

    def parts(exact):
        hi = exact.astype(BF16).astype(F32)
        rest = exact - hi
        mid = rest.astype(BF16).astype(F32)
        low = rest - mid
        return jnp.where(
            lane < heads, hi, jnp.where(lane < 2 * heads, mid, jnp.where(lane < 3 * heads, low, 0.0))
        )

    ones = ((lane >= 3 * heads) & (lane < 3 * heads + 3)).astype(F32)

    def decay_of(step, carry):
        block = lax.rem(me - step + ring, ring)
        summed = lax.dot_general(later, thrice(block), NT, preferred_element_type=F32)
        after = between[...]
        key_extra[block] = (parts((summed[:rows] + after) * root) + ones).astype(BF16)
        between[...] = after + summed[rows : rows + 1]
        return carry

    def decay_own():
        between[...] = -lax.dot_general(later, thrice(me), NT, preferred_element_type=F32)[rows : rows + 1]
        decay_of(0, 0)

    def query_extras(first, end):
        own_sum = lax.dot_general(sofar, thrice(me), NT, preferred_element_type=F32)[:rows]
        own_parts = parts(own_sum * root).astype(BF16)
        pick_row = lax.broadcasted_iota(jnp.int32, (dim, dim), 0)
        pick_lane = lax.broadcasted_iota(jnp.int32, (dim, dim), 1)

        def query_extra(h, carry):
            pick = ((pick_row == h + heads * (pick_lane - 3 * heads)) & (pick_lane >= 3 * heads)
                    & (pick_lane < 3 * heads + 3)).astype(F32).astype(BF16)
            moved = jnp.dot(own_parts, pick, preferred_element_type=F32)
            hot = ((lane == h) | (lane == h + heads) | (lane == h + 2 * heads)).astype(F32)
            place_rows = pl.ds(pl.multiple_of(lax.rem(h, share) * rows, rows), rows)
            queries[lax.div(h, share), place_rows, dim:] = (moved + hot).astype(BF16)
            return carry

        lax.fori_loop(first, end, query_extra, 0)

    def query_group(g, carry):
        at = pl.multiple_of(lax.rem(g, groups // 2) * dim * share, dim * share)
        weight = query_all[lax.div(g, groups // 2), :, pl.ds(at, dim * share)]
        part = jnp.dot(tokens[...], weight, preferred_element_type=F32).astype(BF16)
        for h in range(share):
            queries[g, h * rows : (h + 1) * rows, :dim] = part[:, h * dim : (h + 1) * dim]
        return carry

    scale = math.log2(math.e) / root
    breadth = share * rows

    def attend(blocks, some_groups, diagonal=False):
        key_rows = rows * len(blocks)
        for g in some_groups:
            key_part = jnp.concatenate(
                [jnp.concatenate([keys[block, g], key_extra[block]], axis=1) for block in blocks], axis=0
            )
            value_part = jnp.concatenate([values[block, g] for block in blocks], axis=0)
            score = lax.dot_general(key_part, queries[g], NT, preferred_element_type=F32)
            if diagonal:
                key_at = lax.broadcasted_iota(jnp.int32, (key_rows, breadth), 0)
                query_at = lax.broadcasted_iota(jnp.int32, (key_rows, breadth), 1)
                for h in range(share - 1, 0, -1):
                    query_at = jnp.where(query_at >= h * rows, query_at - h * rows, query_at)
                score = jnp.where(key_at <= query_at, score, -jnp.inf)
                peak = jnp.max(score, axis=0, keepdims=True)
            else:
                old = peaks[g]
                peak = jnp.maximum(old, jnp.max(score, axis=0, keepdims=True))
            weight = jnp.exp2((score - peak) * scale)
            total = jnp.sum(weight, axis=0, keepdims=True)
            mixed = lax.dot_general(value_part, weight.astype(BF16), TN, preferred_element_type=F32)
            peaks[g] = peak
            if diagonal:
                sums[g] = total
                totals[g] = mixed
            else:
                fade = jnp.exp2((old - peak) * scale)
                sums[g] = sums[g] * fade + total
                totals[g] = totals[g] * fade + mixed

    def attend_own(n, carry):
        attend((me,), (2 * n, 2 * n + 1), diagonal=True)
        return carry

    def unit(u, carry):
        pair = lax.div(u, 2)
        some = (2 * lax.rem(u, 2), 2 * lax.rem(u, 2) + 1)
        over = (pair == 2) | (pair == 3) | (pair == 5)
        step = jnp.where(pair < 2, 2 * pair + 1, jnp.where(pair < 4, 2 * pair - 3, jnp.where(pair < 6, 5, 7)))
        one = jnp.where(over, me + step - ring, me - step)
        two = jnp.where(pair == 6, me + step - ring, jnp.where(over, me + step + 1 - ring, me - step - 1))

        @pl.when((one >= 0) & (two >= 0))
        def _():
            attend((one, two), some)

        @pl.when(((one >= 0) | (two >= 0)) & ((one < 0) | (two < 0)))
        def _():
            attend((jnp.maximum(one, two),), some)

        return carry

    gather_keys.begin()
    for fetch in fetches:
        fetch.wait()
    visits(lambda copy: copy.start())
    gather_values.begin()
    gate(tokens, me)
    gather_keys.first()
    gather_values.first()
    decay_own()
    gather_keys.second()
    gather_values.second()
    gather_keys.third()
    gather_values.third()
    gather_keys.fourth()
    gather_left.begin()
    gather_right.begin()
    gather_keys.complete()
    meet(DOWN, 0)
    meet(UP, 0)
    query_extras(0, 1)
    launch_part(KEYS, DOWN, 0)
    launch_part(KEYS, UP, 0)
    gather_values.fourth()
    meet(UP, 1)
    meet_gates(UP)
    launch(GATES, UP)
    meet(DOWN, 1)
    launch_part(KEYS, UP, 1)
    meet_gates(DOWN)
    launch_part(KEYS, DOWN, 1)
    gather_values.complete()
    launch(GATES, DOWN)
    meet_values(UP, 0)
    meet_values(DOWN, 0)
    query_extras(1, 2)
    launch_part(VALUES, UP, 0)
    launch_part(VALUES, DOWN, 0)
    meet_values(UP, 1)
    meet_values(DOWN, 1)
    query_extras(2, 3)
    launch_part(VALUES, UP, 1)
    launch_part(VALUES, DOWN, 1)
    gather_left.first()
    relay(GATES, 2)
    relay(KEYS, 2)
    gather_right.first()
    query_extras(3, heads)
    relay(GATES, 3)
    relay(VALUES, 2)
    project(tokens, key_all, keys, me)
    project(tokens, value_all, values, me)
    gather_left.second()
    relay(GATES, 4)
    relay(KEYS, 3)
    gather_keys.drain()
    gather_values.drain()
    lax.fori_loop(1, 4, decay_of, 0)
    gather_right.second()
    lax.fori_loop(4, 5, decay_of, 0)
    relay(GATES, 5)
    relay(VALUES, 3)
    gather_left.third()
    visits(lambda copy: copy.wait_send())
    lax.fori_loop(5, 6, decay_of, 0)
    relay(GATES, 6)
    relay(KEYS, 4)
    gather_left.fourth()
    gather_right.third()
    lax.fori_loop(6, 7, decay_of, 0)
    gather_left.complete()
    lax.fori_loop(0, groups // 2, query_group, 0)
    gather_right.fourth()
    lax.fori_loop(0, groups // 4, attend_own, 0)
    relay(GATES, 7)
    relay(VALUES, 4)
    gather_right.complete()
    lax.fori_loop(groups // 2, groups, query_group, 0)
    lax.fori_loop(groups // 4, groups // 2, attend_own, 0)
    relay(GATES, 8)
    relay(KEYS, 5)
    lax.fori_loop(7, ring, decay_of, 0, unroll=3)
    lax.fori_loop(0, 2, unit, 0)
    relay(VALUES, 5)
    lax.fori_loop(2, 4, unit, 0)

    def steady(step, carry):
        done = 5 * (step - 6) + 4
        relay(KEYS, step)
        lax.fori_loop(done, done + 3, unit, 0)
        relay(VALUES, step)
        lax.fori_loop(done + 3, done + 5, unit, 0)
        return carry

    lax.fori_loop(6, half, steady, 0)
    gather_left.drain()
    gather_right.drain()
    relay(KEYS, half)

    @pl.when(me >= half)
    def _():
        block = me - half
        for g in range(groups):
            key_part = jnp.concatenate([keys[block, g], key_extra[block]], axis=1)
            score = lax.dot_general(key_part, queries[g], NT, preferred_element_type=F32)
            old = peaks[g]
            peak = jnp.maximum(old, jnp.max(score, axis=0, keepdims=True))
            weight = jnp.exp2((score - peak) * scale)
            fade = jnp.exp2((old - peak) * scale)
            sums[g] = sums[g] * fade + jnp.sum(weight, axis=0, keepdims=True)
            totals[g] = totals[g] * fade
            chances[g] = weight.astype(BF16)

    relay(VALUES, half)

    @pl.when(me >= half)
    def _():
        for g in range(groups):
            totals[g] += lax.dot_general(values[me - half, g], chances[g], TN, preferred_element_type=F32)

    for g in range(groups):
        mixed = (totals[g] / sums[g]).T
        for h in range(share):
            at = (g * share + h) * dim
            out[:, at : at + dim] = mixed[h * rows : (h + 1) * rows].astype(BF16)

    for kind in (KEYS, VALUES, GATES):
        for way in (UP, DOWN):

            @pl.when(passed(kind, way, last[kind, way] - 1))
            def _():
                hop(kind, way, last[kind, way], me).wait_send()


def on_device(tokens, query_weight, key_weight, value_weight, forget_weight, forget_bias):
    token_rows = tokens[0]
    rows, width = token_rows.shape
    ring = lax.axis_size("sp")
    heads = forget_weight.shape[1]
    dim = query_weight.shape[1] // heads
    groups = key_weight.shape[1] // dim
    share = heads // groups
    wide = -(-rows // 128) * 128
    vmem = pl.BlockSpec(memory_space=pltpu.VMEM)
    inputs = (token_rows, query_weight, key_weight, value_weight, forget_weight.T, forget_bias[None, :])
    inputs = tuple(pltpu.with_memory_space_constraint(a, pltpu.HBM) for a in inputs)
    mixed = pl.pallas_call(
        kernel,
        out_shape=jax.ShapeDtypeStruct((rows, heads * dim), BF16),
        in_specs=[pl.BlockSpec(memory_space=pltpu.HBM)] * 6,
        out_specs=vmem,
        scratch_shapes=[
            pltpu.VMEM((rows, width), BF16),
            pltpu.VMEM((heads, width), BF16),
            pltpu.VMEM((1, heads), F32),
            pltpu.VMEM((2, rows, width), BF16),
            pltpu.VMEM((1, dim), F32),
            pltpu.VMEM((groups, rows, share * rows), BF16),
            pltpu.VMEM((2, width, heads * dim // 2), BF16),
            pltpu.VMEM((width, groups * dim), BF16),
            pltpu.VMEM((width, groups * dim), BF16),
            pltpu.VMEM((ring, groups, rows, dim), BF16),
            pltpu.VMEM((ring, groups, rows, dim), BF16),
            pltpu.VMEM((ring, heads, wide), BF16),
            pltpu.VMEM((ring, rows, dim), BF16),
            pltpu.VMEM((groups, share * rows, 2 * dim), BF16),
            pltpu.VMEM((groups, dim, share * rows), F32),
            pltpu.VMEM((groups, 1, share * rows), F32),
            pltpu.VMEM((groups, 1, share * rows), F32),
            pltpu.SemaphoreType.DMA((4,)),
            pltpu.SemaphoreType.DMA((4, len(GROUPS))),
            pltpu.SemaphoreType.DMA((4,)),
            pltpu.SemaphoreType.DMA((4,)),
            pltpu.SemaphoreType.DMA((3, 2, 2)),
            pltpu.SemaphoreType.DMA((3, 2, ring // 2)),
            pltpu.SemaphoreType.DMA((2, 2)),
            pltpu.SemaphoreType.DMA((2, 2)),
            pltpu.SemaphoreType.DMA((7,)),
        ],
        compiler_params=pltpu.CompilerParams(
            collective_id=0, has_side_effects=True, vmem_limit_bytes=32 * 2**20
        ),
    )(*inputs)
    return mixed[None]


def solution(mesh):
    placed = (P("dp", "sp", None), P("dp", None), P("dp", None), P("dp", None), P(), P())
    return jax.shard_map(
        on_device, mesh=mesh, in_specs=placed, out_specs=P("dp", "sp", None), check_vma=False
    )
```

```python
import functools
import math

import jax
import jax.numpy as jnp
from jax import lax
from jax.experimental import pallas as pl
from jax.experimental.pallas import tpu as pltpu
from jax.sharding import PartitionSpec as P

BF16 = jnp.bfloat16
F32 = jnp.float32
MESH = pl.DeviceIdType.MESH
SIDE = 4
KEYS, VALUES, GATES = 0, 1, 2
UP, DOWN = 0, 1
NT = (((1,), (1,)), ((), ()))
TN = (((0,), (0,)), ((), ()))

GROUPS = [
    [("W", 3, 0), ("W", 0, 3)],
    [("W", 1, 0), ("W", 0, 1)],
    [("A", 3, 3), ("A", 1, 3), ("B", 3, 3), ("B", 3, 1)],
    [("W", 2, 0), ("W", 0, 2)],
    [("A", 3, 1), ("A", 1, 1), ("B", 1, 3), ("B", 1, 1)],
    [("A", 2, 3), ("B", 3, 2)],
    [("A", 3, 2), ("A", 1, 2), ("B", 2, 3), ("B", 2, 1), ("A", 2, 1), ("B", 1, 2)],
    [("A", 2, 2), ("B", 2, 2)],
]
OWN = ("W", 0, 0)
ITEM = {key: n for n, group in enumerate(GROUPS) for key in group}


def copy_rows(part, depth):
    return depth if part == "W" else depth // 2


class Gather:
    def __init__(self, number, shard, full, sends, receives, pair_sends, pair_receives, place):
        self.number, self.shard, self.full = number, shard, full
        self.sems = (sends, receives, pair_sends, pair_receives)
        self.place = place
        self.depth = shard.shape[0]
        self.sent = 0

    def slot(self, a, b, other=False):
        x, y, core, turn = self.place
        if other:
            core, turn = 1 - core, -turn
        across = lax.rem(x + turn * a + 2 * SIDE, SIDE)
        along = lax.rem(y + turn * b + 2 * SIDE, SIDE)
        return (along * SIDE + across) * 2 + core

    def rows(self, key, other=False):
        part, a, b = key
        first = self.slot(a, b, other) * self.depth
        count = copy_rows(part, self.depth)
        if part == "B":
            first = first + count
        return self.full.at[pl.ds(pl.multiple_of(first, count), count)]

    def copy(self, key, received, target):
        sends, receives = self.sems[:2]
        n = ITEM[received]
        view = self.rows(key)
        return pltpu.make_async_remote_copy(
            src_ref=view,
            dst_ref=view,
            send_sem=sends.at[self.number],
            recv_sem=receives.at[self.number, n],
            device_id={"dp": target},
            device_id_type=MESH,
        )

    def send(self, key, dx, dy):
        part, a, b = key
        received = (part, (a - dx) % SIDE, (b - dy) % SIDE)
        copy = self.copy(key, received, self.slot(dx, dy))
        copy.start()
        self.sent += copy_rows(part, self.depth)

    def wait(self, group):
        rows = sum(copy_rows(key[0], self.depth) for key in GROUPS[group])
        self.bulk(rows, self.sems[0].at[self.number], self.sems[1].at[self.number, group]).wait_recv()

    def pair_copy(self, a, b, other=False):
        x, y, core, turn = self.place
        view = self.rows(("W", a, b), other)
        return pltpu.make_async_remote_copy(
            src_ref=view,
            dst_ref=view,
            send_sem=self.sems[2].at[self.number],
            recv_sem=self.sems[3].at[self.number],
            device_id={"dp": (y * SIDE + x) * 2 + 1 - core},
            device_id_type=MESH,
        )

    def share(self, a, b):
        self.pair_copy(a, b).start()

    def fetch(self, local_sem):
        self.fetched = pltpu.make_async_copy(self.shard, self.rows(OWN), local_sem)
        self.fetched.start()

    def begin(self):
        self.fetched.wait()
        for dx, dy in ((1, 0), (0, 1), (-1, 0), (0, -1)):
            self.send(OWN, dx, dy)
        self.share(0, 0)

    def first(self):
        self.wait(0)
        self.send(("W", 3, 0), 1, 0)
        self.send(("W", 0, 3), 0, 1)
        for a in (3, 1):
            if a == 1:
                self.wait(1)
            for way in (1, -1):
                self.send(("A", a, 0), 0, way)
                self.send(("B", 0, a), way, 0)
            self.share(a, 0)
            self.share(0, a)

    def second(self):
        self.wait(2)
        for a in (3, 1):
            self.send(("A", a, 3), 0, 1)
            self.send(("B", 3, a), 1, 0)
        self.wait(3)
        for way in (1, -1):
            self.send(("A", 2, 0), 0, way)
            self.send(("B", 0, 2), way, 0)
        self.share(2, 0)
        self.share(0, 2)
        self.wait(4)
        for a in (3, 1):
            for b in (3, 1):
                self.share(a, b)

    def third(self):
        self.wait(5)
        self.send(("A", 2, 3), 0, 1)
        self.send(("B", 3, 2), 1, 0)
        self.wait(6)
        for a in (3, 1):
            self.share(2, a)
            self.share(a, 2)

    def fourth(self):
        self.wait(7)
        self.share(2, 2)

    def bulk(self, rows, send_sem, receive_sem):
        view = self.full.at[pl.ds(0, rows)]
        return pltpu.make_async_remote_copy(
            src_ref=view,
            dst_ref=view,
            send_sem=send_sem,
            recv_sem=receive_sem,
            device_id={"dp": self.slot(1, 0)},
            device_id_type=MESH,
        )

    def complete(self):
        n = self.number
        self.bulk(SIDE * SIDE * self.depth, self.sems[2].at[n], self.sems[3].at[n]).wait_recv()

    def drain(self):
        n = self.number
        self.bulk(self.sent, self.sems[0].at[n], self.sems[3].at[n]).wait_send()
        self.bulk(SIDE * SIDE * self.depth, self.sems[2].at[n], self.sems[3].at[n]).wait_send()


def kernel(
    tokens_in, query_shard, key_shard, value_shard, forget_in, bias_in, out,
    tokens, forget_weight, forget_bias, near, between, chances, query_all, key_all, value_all, keys, values, gates, key_extra, queries, totals, peaks, sums,
    sends, receives, pair_sends, pair_receives, ring_sends, ring_receives, near_sends, near_receives, local_sems,
):
    ring = lax.axis_size("sp")
    half = ring // 2
    me = lax.axis_index("sp")
    mine = lax.axis_index("dp")
    core = lax.rem(mine, 2)
    x = lax.rem(lax.div(mine, 2), SIDE)
    y = lax.div(mine, 2 * SIDE)
    place = (x, y, core, 1 - 2 * core)
    rows = tokens.shape[0]
    heads = forget_weight.shape[0]
    groups, dim = keys.shape[1], keys.shape[3]
    share = heads // groups
    root = math.sqrt(dim)

    part_width = query_all.shape[2]
    gather_keys, gather_values, gather_left, gather_right = (
        Gather(n, shard, full, sends, receives, pair_sends, pair_receives, place)
        for n, (shard, full) in enumerate(
            (
                (key_shard, key_all),
                (value_shard, value_all),
                (query_shard.at[:, pl.ds(0, part_width)], query_all.at[0]),
                (query_shard.at[:, pl.ds(part_width, part_width)], query_all.at[1]),
            )
        )
    )

    above, below = lax.rem(me + 1, ring), lax.rem(me + ring - 1, ring)
    barrier = pltpu.get_barrier_semaphore()
    for dx, dy in ((1, 0), (0, 1), (-1, 0), (0, -1)):
        pl.semaphore_signal(
            barrier, inc=1, device_id={"dp": gather_keys.slot(dx, dy)}, device_id_type=MESH
        )
    pl.semaphore_signal(barrier, inc=1, device_id={"dp": mine + 1 - 2 * core}, device_id_type=MESH)
    for neighbour in (above, below):
        pl.semaphore_signal(barrier, inc=1, device_id={"sp": neighbour}, device_id_type=MESH)
    gather_keys.fetch(local_sems.at[0])
    fetches = [
        pltpu.make_async_copy(source, target, local_sems.at[n + 3])
        for n, (source, target) in enumerate(
            ((tokens_in, tokens), (forget_in, forget_weight), (bias_in, forget_bias))
        )
    ]
    for fetch in fetches:
        fetch.start()
    gather_values.fetch(local_sems.at[1])
    gather_left.fetch(local_sems.at[2])
    gather_right.fetch(local_sems.at[6])
    pl.semaphore_wait(barrier, 7)

    buffers = {KEYS: keys, VALUES: values, GATES: gates}
    last = {
        (KEYS, UP): half, (KEYS, DOWN): half,
        (VALUES, UP): half, (VALUES, DOWN): half,
        (GATES, UP): half, (GATES, DOWN): half - 1,
    }

    def hop(kind, way, step, slot):
        view = buffers[kind].at[slot]
        if kind != GATES and step == half:
            view = buffers[kind].at[slot, pl.ds(0, groups - 1) if way == UP else pl.ds(groups - 1, 1)]
        return pltpu.make_async_remote_copy(
            src_ref=view,
            dst_ref=view,
            send_sem=ring_sends.at[kind, way, step % 2],
            recv_sem=ring_receives.at[kind, way, step - 1],
            device_id={"sp": above if way == UP else below},
            device_id_type=MESH,
        )

    def origin(way, step):
        return lax.rem(me - step + ring, ring) if way == UP else lax.rem(me + step, ring)

    def fresh(kind, way, step):
        if way == UP:
            return me >= step
        return (me + step >= ring) | (me + step < last[kind, way])

    def passed(kind, way, step):
        return (me >= step) & (me < ring - 1) if way == UP else fresh(kind, way, step)

    def launch(kind, way):
        @pl.when(passed(kind, way, 1))
        def _():
            hop(kind, way, 2, origin(way, 1)).start()

    def first_hop(kind, way, part, slot):
        view = (
            keys.at[slot, :, pl.ds(part * (rows // 2), rows // 2)]
            if kind == KEYS
            else values.at[slot, pl.ds(part * (groups // 2), groups // 2)]
        )
        return pltpu.make_async_remote_copy(
            src_ref=view,
            dst_ref=view,
            send_sem=ring_sends.at[kind, way, part],
            recv_sem=ring_receives.at[kind, way, part],
            device_id={"sp": above if way == UP else below},
            device_id_type=MESH,
        )

    def launch_part(kind, way, part):
        @pl.when(passed(kind, way, 1))
        def _():
            first_hop(kind, way, part, origin(way, 1)).start()

    def relay(kind, step):
        for way in (UP, DOWN):
            final = last[kind, way]
            slot = origin(way, step)
            if step > final:
                continue
            begins = step == 2 and kind != GATES

            @pl.when(fresh(kind, way, step))
            def _():
                if begins:
                    first_hop(kind, way, 0, slot).wait_recv()
                    first_hop(kind, way, 1, slot).wait_recv()
                else:
                    hop(kind, way, step, slot).wait_recv()

            if begins:

                @pl.when(passed(kind, way, 1))
                def _():
                    first_hop(kind, way, 0, slot).wait_send()
                    first_hop(kind, way, 1, slot).wait_send()

            elif step > 3 or (step == 3 and kind == GATES):

                @pl.when(passed(kind, way, step - 2))
                def _():
                    hop(kind, way, step - 1, slot).wait_send()

            if step < final:

                @pl.when(passed(kind, way, step))
                def _():
                    hop(kind, way, step + 1, slot).start()

    def visit(way, part):
        these = pl.ds(part * (rows // 2), rows // 2)
        return pltpu.make_async_remote_copy(
            src_ref=tokens.at[these],
            dst_ref=near.at[way, these],
            send_sem=near_sends.at[way, part],
            recv_sem=near_receives.at[way, part],
            device_id={"sp": above if way == UP else below},
            device_id_type=MESH,
        )

    def visits(act):
        for part in (0, 1):
            for way, goes in ((UP, me < ring - 1), (DOWN, me < half)):

                @pl.when(goes)
                def _():
                    act(visit(way, part))

    comes = {UP: me >= 1, DOWN: (me == ring - 1) | (me < half - 1)}

    def meet(way, part):
        @pl.when(comes[way])
        def _():
            visit(way, part).wait_recv()
            project(near.at[way], key_all, keys, origin(way, 1), part * (rows // 2), rows // 2)

    def meet_gates(way):
        @pl.when(comes[way])
        def _():
            gate(near.at[way], origin(way, 1))

    def meet_values(way, part):
        @pl.when(comes[way])
        def _():
            project(near.at[way], value_all, values, origin(way, 1), some=(part, part + 1))

    wide = gates.shape[2]
    eye = (
        lax.broadcasted_iota(jnp.int32, (rows, wide), 0) == lax.broadcasted_iota(jnp.int32, (rows, wide), 1)
    ).astype(F32).astype(BF16)

    def gate(source, block):
        bias_at = lax.broadcasted_iota(jnp.int32, (heads, heads), 0) == lax.broadcasted_iota(jnp.int32, (heads, heads), 1)
        bias = jnp.sum(jnp.where(bias_at, forget_bias[...], 0.0), axis=1, keepdims=True)
        gate_input = lax.dot_general(forget_weight[...], source[...], NT, preferred_element_type=F32) + bias
        log_gate = (jnp.minimum(gate_input, 0.0) - jnp.log1p(jnp.exp(-jnp.abs(gate_input)))).astype(BF16)
        gates[block] = jnp.dot(log_gate, eye, preferred_element_type=F32).astype(BF16)

    def project(source, weight, buffer, block, first=0, count=rows, some=(0, groups // 2)):
        def one(g, carry):
            columns = pl.ds(pl.multiple_of(g * dim * 2, dim * 2), dim * 2)
            these = source[pl.ds(first, count), :]
            part = jnp.dot(these, weight[:, columns], preferred_element_type=F32).astype(BF16)
            buffer[block, 2 * g, pl.ds(first, count)] = part[:, :dim]
            buffer[block, 2 * g + 1, pl.ds(first, count)] = part[:, dim:]
            return carry

        lax.fori_loop(some[0], some[1], one, 0)

    lane = lax.broadcasted_iota(jnp.int32, (rows, dim), 1)
    tall = rows + 8
    down = lax.broadcasted_iota(jnp.int32, (tall, wide), 0)
    right = lax.broadcasted_iota(jnp.int32, (tall, wide), 1)
    later = ((right > down) | (down >= rows)).astype(F32).astype(BF16)
    sofar = ((right <= down) & (down < rows)).astype(F32).astype(BF16)

    def thrice(block):
        g = gates[block]
        return jnp.concatenate([g, g, g, jnp.zeros((dim - 3 * heads, wide), BF16)], axis=0)

    def parts(exact):
        hi = exact.astype(BF16).astype(F32)
        rest = exact - hi
        mid = rest.astype(BF16).astype(F32)
        low = rest - mid
        return jnp.where(
            lane < heads, hi, jnp.where(lane < 2 * heads, mid, jnp.where(lane < 3 * heads, low, 0.0))
        )

    ones = ((lane >= 3 * heads) & (lane < 3 * heads + 3)).astype(F32)

    def decay_of(step, carry):
        block = lax.rem(me - step + ring, ring)
        summed = lax.dot_general(later, thrice(block), NT, preferred_element_type=F32)
        after = between[...]
        key_extra[block] = (parts((summed[:rows] + after) * root) + ones).astype(BF16)
        between[...] = after + summed[rows : rows + 1]
        return carry

    def decay_own():
        between[...] = -lax.dot_general(later, thrice(me), NT, preferred_element_type=F32)[rows : rows + 1]
        decay_of(0, 0)

    def query_extras(first, end):
        own_sum = lax.dot_general(sofar, thrice(me), NT, preferred_element_type=F32)[:rows]
        own_parts = parts(own_sum * root).astype(BF16)
        pick_row = lax.broadcasted_iota(jnp.int32, (dim, dim), 0)
        pick_lane = lax.broadcasted_iota(jnp.int32, (dim, dim), 1)

        def query_extra(h, carry):
            pick = ((pick_row == h + heads * (pick_lane - 3 * heads)) & (pick_lane >= 3 * heads)
                    & (pick_lane < 3 * heads + 3)).astype(F32).astype(BF16)
            moved = jnp.dot(own_parts, pick, preferred_element_type=F32)
            hot = ((lane == h) | (lane == h + heads) | (lane == h + 2 * heads)).astype(F32)
            place_rows = pl.ds(pl.multiple_of(lax.rem(h, share) * rows, rows), rows)
            queries[lax.div(h, share), place_rows, dim:] = (moved + hot).astype(BF16)
            return carry

        lax.fori_loop(first, end, query_extra, 0)

    def query_group(g, carry):
        at = pl.multiple_of(lax.rem(g, groups // 2) * dim * share, dim * share)
        weight = query_all[lax.div(g, groups // 2), :, pl.ds(at, dim * share)]
        part = jnp.dot(tokens[...], weight, preferred_element_type=F32).astype(BF16)
        for h in range(share):
            queries[g, h * rows : (h + 1) * rows, :dim] = part[:, h * dim : (h + 1) * dim]
        return carry

    scale = math.log2(math.e) / root
    breadth = share * rows

    def attend(blocks, some_groups, diagonal=False):
        key_rows = rows * len(blocks)
        for g in some_groups:
            key_part = jnp.concatenate(
                [jnp.concatenate([keys[block, g], key_extra[block]], axis=1) for block in blocks], axis=0
            )
            value_part = jnp.concatenate([values[block, g] for block in blocks], axis=0)
            score = lax.dot_general(key_part, queries[g], NT, preferred_element_type=F32)
            if diagonal:
                key_at = lax.broadcasted_iota(jnp.int32, (key_rows, breadth), 0)
                query_at = lax.broadcasted_iota(jnp.int32, (key_rows, breadth), 1)
                for h in range(share - 1, 0, -1):
                    query_at = jnp.where(query_at >= h * rows, query_at - h * rows, query_at)
                score = jnp.where(key_at <= query_at, score, -jnp.inf)
                peak = jnp.max(score, axis=0, keepdims=True)
            else:
                old = peaks[g]
                peak = jnp.maximum(old, jnp.max(score, axis=0, keepdims=True))
            weight = jnp.exp2((score - peak) * scale)
            total = jnp.sum(weight, axis=0, keepdims=True)
            mixed = lax.dot_general(value_part, weight.astype(BF16), TN, preferred_element_type=F32)
            peaks[g] = peak
            if diagonal:
                sums[g] = total
                totals[g] = mixed
            else:
                fade = jnp.exp2((old - peak) * scale)
                sums[g] = sums[g] * fade + total
                totals[g] = totals[g] * fade + mixed

    def attend_own(n, carry):
        attend((me,), (2 * n, 2 * n + 1), diagonal=True)
        return carry

    def unit(u, carry):
        pair = lax.div(u, 2)
        some = (2 * lax.rem(u, 2), 2 * lax.rem(u, 2) + 1)
        over = (pair == 2) | (pair == 3) | (pair == 5)
        step = jnp.where(pair < 2, 2 * pair + 1, jnp.where(pair < 4, 2 * pair - 3, jnp.where(pair < 6, 5, 7)))
        one = jnp.where(over, me + step - ring, me - step)
        two = jnp.where(pair == 6, me + step - ring, jnp.where(over, me + step + 1 - ring, me - step - 1))

        @pl.when((one >= 0) & (two >= 0))
        def _():
            attend((one, two), some)

        @pl.when(((one >= 0) | (two >= 0)) & ((one < 0) | (two < 0)))
        def _():
            attend((jnp.maximum(one, two),), some)

        return carry

    gather_keys.begin()
    for fetch in fetches:
        fetch.wait()
    visits(lambda copy: copy.start())
    gather_values.begin()
    gate(tokens, me)
    gather_keys.first()
    gather_values.first()
    decay_own()
    gather_keys.second()
    gather_values.second()
    gather_keys.third()
    gather_values.third()
    gather_keys.fourth()
    gather_left.begin()
    gather_right.begin()
    gather_keys.complete()
    meet(DOWN, 0)
    meet(UP, 0)
    query_extras(0, 1)
    launch_part(KEYS, DOWN, 0)
    launch_part(KEYS, UP, 0)
    gather_values.fourth()
    meet(UP, 1)
    meet_gates(UP)
    launch(GATES, UP)
    meet(DOWN, 1)
    launch_part(KEYS, UP, 1)
    meet_gates(DOWN)
    launch_part(KEYS, DOWN, 1)
    gather_values.complete()
    launch(GATES, DOWN)
    meet_values(UP, 0)
    meet_values(DOWN, 0)
    query_extras(1, 2)
    launch_part(VALUES, UP, 0)
    launch_part(VALUES, DOWN, 0)
    meet_values(UP, 1)
    meet_values(DOWN, 1)
    query_extras(2, 3)
    launch_part(VALUES, UP, 1)
    launch_part(VALUES, DOWN, 1)
    gather_left.first()
    relay(GATES, 2)
    relay(KEYS, 2)
    gather_right.first()
    query_extras(3, heads)
    relay(GATES, 3)
    relay(VALUES, 2)
    project(tokens, key_all, keys, me)
    project(tokens, value_all, values, me)
    gather_left.second()
    relay(GATES, 4)
    relay(KEYS, 3)
    gather_keys.drain()
    gather_values.drain()
    lax.fori_loop(1, 4, decay_of, 0)
    gather_right.second()
    lax.fori_loop(4, 5, decay_of, 0)
    relay(GATES, 5)
    relay(VALUES, 3)
    gather_left.third()
    visits(lambda copy: copy.wait_send())
    lax.fori_loop(5, 6, decay_of, 0)
    relay(GATES, 6)
    relay(KEYS, 4)
    gather_left.fourth()
    gather_right.third()
    lax.fori_loop(6, 7, decay_of, 0)
    gather_left.complete()
    lax.fori_loop(0, groups // 2, query_group, 0)
    gather_right.fourth()
    lax.fori_loop(0, groups // 4, attend_own, 0)
    relay(GATES, 7)
    relay(VALUES, 4)
    gather_right.complete()
    lax.fori_loop(groups // 2, groups, query_group, 0)
    lax.fori_loop(groups // 4, groups // 2, attend_own, 0)
    relay(GATES, 8)
    relay(KEYS, 5)
    lax.fori_loop(7, ring, decay_of, 0, unroll=3)
    lax.fori_loop(0, 2, unit, 0)
    relay(VALUES, 5)
    lax.fori_loop(2, 5, unit, 0)

    def finish():
        for g in range(groups):
            mixed = (totals[g] / sums[g]).T
            for h in range(share):
                at = (g * share + h) * dim
                out[:, at : at + dim] = mixed[h * rows : (h + 1) * rows].astype(BF16)

    for step in (6, half - 1):
        done = 5 * (step - 6) + 5
        relay(KEYS, step)
        lax.fori_loop(done, done + 2, unit, 0)
        if step == half - 1:

            @pl.when(me < half - 1)
            def _():
                finish()

        relay(VALUES, step)
        lax.fori_loop(done + 2, min(done + 5, 2 * (half - 1)), unit, 0)

    gather_left.drain()
    gather_right.drain()
    relay(KEYS, half)

    @pl.when(me >= half)
    def _():
        block = me - half
        for g in range(groups):
            key_part = jnp.concatenate([keys[block, g], key_extra[block]], axis=1)
            score = lax.dot_general(key_part, queries[g], NT, preferred_element_type=F32)
            old = peaks[g]
            peak = jnp.maximum(old, jnp.max(score, axis=0, keepdims=True))
            weight = jnp.exp2((score - peak) * scale)
            fade = jnp.exp2((old - peak) * scale)
            sums[g] = sums[g] * fade + jnp.sum(weight, axis=0, keepdims=True)
            totals[g] = totals[g] * fade
            chances[g] = weight.astype(BF16)

    relay(VALUES, half)

    @pl.when(me >= half)
    def _():
        for g in range(groups):
            totals[g] += lax.dot_general(values[me - half, g], chances[g], TN, preferred_element_type=F32)

    @pl.when(me >= half - 1)
    def _():
        finish()

    for kind in (KEYS, VALUES, GATES):
        for way in (UP, DOWN):

            @pl.when(passed(kind, way, last[kind, way] - 1))
            def _():
                hop(kind, way, last[kind, way], me).wait_send()


def on_device(tokens, query_weight, key_weight, value_weight, forget_weight, forget_bias):
    token_rows = tokens[0]
    rows, width = token_rows.shape
    ring = lax.axis_size("sp")
    heads = forget_weight.shape[1]
    dim = query_weight.shape[1] // heads
    groups = key_weight.shape[1] // dim
    share = heads // groups
    wide = -(-rows // 128) * 128
    vmem = pl.BlockSpec(memory_space=pltpu.VMEM)
    inputs = (token_rows, query_weight, key_weight, value_weight, forget_weight.T, forget_bias[None, :])
    inputs = tuple(pltpu.with_memory_space_constraint(a, pltpu.HBM) for a in inputs)
    mixed = pl.pallas_call(
        kernel,
        out_shape=jax.ShapeDtypeStruct((rows, heads * dim), BF16),
        in_specs=[pl.BlockSpec(memory_space=pltpu.HBM)] * 6,
        out_specs=vmem,
        scratch_shapes=[
            pltpu.VMEM((rows, width), BF16),
            pltpu.VMEM((heads, width), BF16),
            pltpu.VMEM((1, heads), F32),
            pltpu.VMEM((2, rows, width), BF16),
            pltpu.VMEM((1, dim), F32),
            pltpu.VMEM((groups, rows, share * rows), BF16),
            pltpu.VMEM((2, width, heads * dim // 2), BF16),
            pltpu.VMEM((width, groups * dim), BF16),
            pltpu.VMEM((width, groups * dim), BF16),
            pltpu.VMEM((ring, groups, rows, dim), BF16),
            pltpu.VMEM((ring, groups, rows, dim), BF16),
            pltpu.VMEM((ring, heads, wide), BF16),
            pltpu.VMEM((ring, rows, dim), BF16),
            pltpu.VMEM((groups, share * rows, 2 * dim), BF16),
            pltpu.VMEM((groups, dim, share * rows), F32),
            pltpu.VMEM((groups, 1, share * rows), F32),
            pltpu.VMEM((groups, 1, share * rows), F32),
            pltpu.SemaphoreType.DMA((4,)),
            pltpu.SemaphoreType.DMA((4, len(GROUPS))),
            pltpu.SemaphoreType.DMA((4,)),
            pltpu.SemaphoreType.DMA((4,)),
            pltpu.SemaphoreType.DMA((3, 2, 2)),
            pltpu.SemaphoreType.DMA((3, 2, ring // 2)),
            pltpu.SemaphoreType.DMA((2, 2)),
            pltpu.SemaphoreType.DMA((2, 2)),
            pltpu.SemaphoreType.DMA((7,)),
        ],
        compiler_params=pltpu.CompilerParams(
            collective_id=0, has_side_effects=True, vmem_limit_bytes=32 * 2**20
        ),
    )(*inputs)
    return mixed[None]


def solution(mesh):
    placed = (P("dp", "sp", None), P("dp", None), P("dp", None), P("dp", None), P(), P())
    return jax.shard_map(
        on_device, mesh=mesh, in_specs=placed, out_specs=P("dp", "sp", None), check_vma=False
    )
```
